32 devices in a mesh: sp: 8 (over z, y), dp: 4 (over x, core).
Axes of the slice: x: 2, y: 2, z: 4, core: 2. Of those that a mesh axis runs over, the one named last changes fastest.
Arguments:
- residual: bfloat16 [4, 1024, 2048], P('dp', 'sp'), may hold values from -6 to 6
- head_input: bfloat16 [4, 1024, 2048], P('dp', 'sp'), may hold values from -6 to 6
- gate_input: bfloat16 [4, 1024, 2048], P('dp', 'sp'), may hold values from -6 to 6
- b_input: bfloat16 [4, 1024, 1024], P('dp', 'sp'), may hold values from -6 to 6
- c_input: bfloat16 [4, 1024, 1024], P('dp', 'sp'), may hold values from -6 to 6
- step_input: bfloat16 [4, 1024, 32], P('dp', 'sp'), may hold values from -4.8 to 4.8
- conv_weight: bfloat16 [4, 2048], replicated, may hold values from -3 to 3
- conv_b_weight: bfloat16 [4, 1024], replicated, may hold values from -3 to 3
- conv_c_weight: bfloat16 [4, 1024], replicated, may hold values from -3 to 3
- step_bias: float32 [32], replicated, may hold values from -1 to 1
- decay_log: float32 [32], replicated, may hold values from -9.92 to -2.99
- skip: float32 [32], replicated, may hold values from 0.5 to 1.5
- norm_gain: float32 [2048], replicated, may hold values from 0.1 to 1.9
- out_weight: bfloat16 [2048, 2048], P('dp'), may hold values from -0.125 to 0.125
- ffn_gain: float32 [2048], replicated, may hold values from 0.1 to 1.9
- shared_gate: bfloat16 [2048, 512], replicated, may hold values from -0.125 to 0.125
- shared_up: bfloat16 [2048, 512], replicated, may hold values from -0.125 to 0.125
- shared_down: bfloat16 [512, 2048], replicated, may hold values from -0.25 to 0.25
- expert_gate: bfloat16 [32, 2048, 512], P(('sp', 'dp')), may hold values from -0.125 to 0.125
- expert_up: bfloat16 [32, 2048, 512], P(('sp', 'dp')), may hold values from -0.125 to 0.125
- expert_down: bfloat16 [32, 512, 2048], P(('sp', 'dp')), may hold values from -0.25 to 0.25
- routes: int32 [4, 1024, 2], P('dp', 'sp'), may hold values from 0 to 31, all different within a row; in each aligned block of 128 rows (0 to 127, 128 to 255, ..., all dimensions but the last counted through in order) at most 16 rows name the same one
- route_weights: float32 [4, 1024, 2], P('dp', 'sp'), may hold values from 0.25 to 1.25
Outputs:
- layer_out: bfloat16 [4, 1024, 2048], P('dp', 'sp')
The draws below stay inside these ranges and needn't reach their ends.
Inputs may be any that keep to these rules, and one draw needn't show every extreme that they name: `routes`: each token names 2 different experts; among the rows of one device no expert is named more than 16 times, a bound that some block reaches.
All inputs are finite; a program needn't handle non-finite values.
Results may differ from the reference program's by a relative error of at most 0.015.
Values may be sent and summed in bfloat16 or wider, within the bound.
No kernel may reach another device: no remote copies, remote signals or barrier semaphores. Data moves between devices by JAX's collectives and lax.ppermute only.
A program may use at most 128 MiB of HBM per device.

```python
import math
import jax
import jax.numpy as jnp
import numpy as np
from jax import lax

D = 2048
HEADS = 32
HEAD_DIM = 64
GROUPS = 8
STATE = 128
CONV_K = 4
BLOCK = 128
EXPERT_FF = 512
SHARED_FF = 512
TOP_K = 2
TOK_DEV = 128
INNER = 2048
SEQS = 4
LENGTH = 1024
EXPERTS = 32
CAP = 16
N_SP = 8
N_DP = 4


def draw_decay_log(key, part):
    first, second, third = jax.random.split(key, 3)
    share = 0.5
    quick = jax.random.uniform(first, (HEADS,), jnp.float32) < share
    slow = jax.random.uniform(second, (HEADS,), jnp.float32, math.log(5e-05), math.log(0.0002))
    fast = jax.random.uniform(third, (HEADS,), jnp.float32, math.log(0.015), math.log(0.05))
    return jnp.where(quick, fast, slow).astype(jnp.float32)


def draw_step_input(key, part):
    first, second = jax.random.split(key)
    count = LENGTH // TOK_DEV
    offset = jax.random.uniform(second, (SEQS, count, 1, HEADS), jnp.float32, -1.2, 1.2)
    noise = jnp.clip(jax.random.normal(first, (SEQS, count, TOK_DEV, HEADS), jnp.float32) * 0.6, -3.5, 3.5)
    return (offset + noise).reshape(SEQS, LENGTH, HEADS).astype(jnp.bfloat16)


def shard_levels(own_key, shape, pieces, least, largest):
    factor_of = 1.0
    for dim, blocks in pieces:
        steps = jax.random.uniform(jax.random.fold_in(jax.random.fold_in(own_key, 6), dim), (blocks,), jnp.float32, least / len(pieces), largest / len(pieces))
        factor_of = factor_of * jnp.repeat(jnp.exp(steps), shape[dim] // blocks).reshape((-1,) + (1,) * (len(shape) - 1 - dim))
    return factor_of


def routed_block(stream_key, own, number, rows, count, top, limit, slope):
    sequence = jax.random.permutation(stream_key, count)
    crowded, ordinary = load_shares(count, rows * top, limit, slope, True), load_shares(count, rows * top, limit, slope, False)
    places = jnp.arange(count)

    def named(lengths, rotation):
        used = int((lengths > 0).sum())
        fixed = max(1, used // 4)
        shifted = fixed + (places - fixed + rotation * (used - fixed)) % max(1, count - fixed)
        return jnp.zeros((count,), jnp.int32).at[sequence[jnp.where(places < fixed, places, shifted)]].set(jnp.asarray(lengths, jnp.int32))

    lengths = jnp.where(number % 4 == 0, named(crowded, number // 4), named(ordinary, number - number // 4 - 1))
    mixed = jax.random.permutation(jax.random.fold_in(own, 3), count)
    donor, receiver = mixed[0:count // 2 * 2:2], mixed[1:count // 2 * 2:2]
    room = jnp.minimum(lengths[donor] - 1, limit - lengths[receiver]) // 2
    room = jnp.where((donor == sequence[0]) | (receiver == sequence[0]) | (lengths[receiver] == 0), 0, jnp.maximum(room, 0))
    shifted = jax.random.randint(jax.random.fold_in(own, 4), (count // 2,), 0, 1 << 20) % (room + 1)
    lengths = lengths.at[donor].add(-shifted).at[receiver].add(shifted)
    labels = jnp.searchsorted(jnp.cumsum(lengths), jnp.arange(rows * top), side="right").astype(jnp.int32)
    listing = labels.reshape(top, rows).T
    listing = listing[jax.random.permutation(jax.random.fold_in(own, 1), rows)]
    rotation = jax.random.randint(jax.random.fold_in(own, 2), (rows, 1), 0, top)
    return jnp.take_along_axis(listing, (jnp.arange(top)[None, :] + rotation) % top, axis=1)


def load_shares(count, total, reach, slope, full):
    loads = [(1 << 20) // math.isqrt(rank ** slope) + 1 for rank in range(1, count + 1)]
    largest = reach if full else min(reach, max(-(-total // count), total * loads[0] // sum(loads)))
    least = 1 if total - largest >= count - 1 else 0
    given, rest = [largest] + [least] * (count - 1), total - largest - least * (count - 1)
    while rest > 0:
        movable = [i for i in range(1, count) if given[i] < largest] or [i for i in range(1, count) if given[i] < reach]
        pool, budget = sum([loads[i] for i in movable]), rest
        for i in movable:
            extra = min(reach - given[i], max(1, budget * loads[i] // pool), rest)
            given[i] = given[i] + extra
            rest = rest - extra
    return np.array(given)


def scatter_about(own_key, extent, scale, bound, pieces=(), kind=jnp.bfloat16):
    values = scale * jax.random.normal(own_key, extent, jnp.float32)
    if pieces:
        values = values * shard_levels(own_key, extent, pieces, -0.22, 0.18)
    return jnp.clip(values, -bound, bound).astype(kind)


def setup_inputs(seed: int = 0) -> dict:
    keys = jax.random.split(jax.random.key(seed), 24)
    residual = scatter_about(keys[0], (SEQS, LENGTH, D), 1.0, 6.0, ((0, 4), (1, 8)))
    head_input = scatter_about(keys[1], (SEQS, LENGTH, INNER), 1.0, 6.0, ((0, 4), (1, 8)))
    gate_input = scatter_about(keys[2], (SEQS, LENGTH, INNER), 1.0, 6.0, ((0, 4), (1, 8)))
    b_input = scatter_about(keys[3], (SEQS, LENGTH, GROUPS * STATE), 1.0, 6.0, ((0, 4), (1, 8)))
    c_input = scatter_about(keys[4], (SEQS, LENGTH, GROUPS * STATE), 1.0, 6.0, ((0, 4), (1, 8)))
    step_input = draw_step_input(jax.random.fold_in(keys[23], 71), 0)
    conv_weight = scatter_about(keys[6], (CONV_K, INNER), 0.5, 3.0)
    conv_b_weight = scatter_about(keys[7], (CONV_K, GROUPS * STATE), 0.5, 3.0)
    conv_c_weight = scatter_about(keys[8], (CONV_K, GROUPS * STATE), 0.5, 3.0)
    step_bias = jnp.clip(jax.random.uniform(keys[9], (HEADS,), jnp.float32, -1.0, 1.0), -1.0, 1.0)
    decay_log = draw_decay_log(jax.random.fold_in(keys[23], 71), 0)
    skip = jnp.clip(jax.random.uniform(keys[11], (HEADS,), jnp.float32, 0.5, 1.5), 0.5, 1.5)
    norm_gain = jnp.clip(1.0 + 0.18 * jax.random.normal(keys[12], (INNER,), jnp.float32), 0.1, 1.9)
    out_weight = scatter_about(keys[13], (INNER, D), INNER ** -0.5, 0.125, ((0, 4),))
    ffn_gain = jnp.clip(1.0 + 0.18 * jax.random.normal(keys[14], (D,), jnp.float32), 0.1, 1.9)
    shared_gate = scatter_about(keys[15], (D, SHARED_FF), D ** -0.5, 0.125)
    shared_up = scatter_about(keys[16], (D, SHARED_FF), D ** -0.5, 0.125)
    shared_down = scatter_about(keys[17], (SHARED_FF, D), SHARED_FF ** -0.5, 0.25)
    expert_gate = scatter_about(keys[18], (EXPERTS, D, EXPERT_FF), D ** -0.5, 0.125, ((0, 32),))
    expert_up = scatter_about(keys[19], (EXPERTS, D, EXPERT_FF), D ** -0.5, 0.125, ((0, 32),))
    expert_down = scatter_about(keys[20], (EXPERTS, EXPERT_FF, D), EXPERT_FF ** -0.5, 0.25, ((0, 32),))
    routes_keys = jax.random.split(jax.random.fold_in(keys[21], 1), SEQS * LENGTH // TOK_DEV)
    routes_turns = jax.random.permutation(jax.random.fold_in(keys[21], 3), SEQS * LENGTH // TOK_DEV)
    routes = jax.vmap(lambda own, number: routed_block(jax.random.fold_in(keys[21], 2), own, number, TOK_DEV, EXPERTS, TOP_K, CAP, 2))(routes_keys, routes_turns).reshape((SEQS, LENGTH, TOP_K))
    route_weights = jnp.clip(0.25 + 1.0 * jax.random.uniform(keys[22], (SEQS, LENGTH, TOP_K), jnp.float32) ** shard_levels(keys[22], (SEQS, LENGTH, TOP_K), ((0, 4), (1, 8)), -0.2, 0.2), 0.25, 1.25)
    return {"residual": residual, "head_input": head_input, "gate_input": gate_input, "b_input": b_input, "c_input": c_input, "step_input": step_input, "conv_weight": conv_weight, "conv_b_weight": conv_b_weight, "conv_c_weight": conv_c_weight, "step_bias": step_bias, "decay_log": decay_log, "skip": skip, "norm_gain": norm_gain, "out_weight": out_weight, "ffn_gain": ffn_gain, "shared_gate": shared_gate, "shared_up": shared_up, "shared_down": shared_down, "expert_gate": expert_gate, "expert_up": expert_up, "expert_down": expert_down, "routes": routes, "route_weights": route_weights}


EPS = 1e-06
HIGH = lax.Precision.HIGHEST

def conv_silu(padded, weight, length):
    total = jnp.zeros((length, padded.shape[1]), jnp.float32)
    for tap in range(weight.shape[0]):
        total = total + padded[tap:tap + length].astype(jnp.float32) * weight[tap].astype(jnp.float32)
    return jax.nn.silu(total)

def block_scan(xs, step, rate, bmat, cmat, block, init):
    length, heads, width = xs.shape
    count = length // block
    logs = (step * rate[None, :]).reshape(count, block, heads)
    weighted = (xs * step[:, :, None]).reshape(count, block, heads, width)
    bb = bmat.reshape(count, block, heads, -1)
    cc = cmat.reshape(count, block, heads, -1)
    cum = jnp.cumsum(logs, axis=1)
    lower = jnp.tril(jnp.ones((block, block), dtype=bool))[None, :, :, None]
    diff = cum[:, :, None, :] - cum[:, None, :, :]
    decay = jnp.where(lower, jnp.exp(jnp.where(lower, diff, 0.0)), 0.0)
    scores = jnp.einsum('clhn,cshn->clsh', cc, bb, precision=HIGH) * decay
    inner = jnp.einsum('clsh,cshp->clhp', scores, weighted, precision=HIGH)
    to_end = jnp.exp(cum[:, -1:, :] - cum)
    states = jnp.einsum('cshn,cshp->chpn', bb * to_end[..., None], weighted, precision=HIGH)
    totals = jnp.exp(cum[:, -1, :])

    def advance(carry, item):
        fresh, factor = item
        return (carry * factor[:, None, None] + fresh, carry)
    last, before = lax.scan(advance, init, (states, totals))
    outer = jnp.einsum('clhn,chpn->clhp', cc * jnp.exp(cum)[..., None], before, precision=HIGH)
    return ((inner + outer).reshape(length, heads, width), last)

def reference(residual, head_input, gate_input, b_input, c_input, step_input, conv_weight, conv_b_weight, conv_c_weight, step_bias, decay_log, skip, norm_gain, out_weight, ffn_gain, shared_gate, shared_up, shared_down, expert_gate, expert_up, expert_down, routes, route_weights):
    taps = jnp.concatenate([conv_weight, conv_b_weight, conv_c_weight], axis=1)
    rate = -jnp.exp(decay_log)
    per_group = HEADS // GROUPS
    span = GROUPS * STATE

    def one_sequence(items):
        x_seq, b_seq, c_seq, s_seq, g_seq, r_seq = items
        rows = jnp.concatenate([x_seq, b_seq, c_seq], axis=1)
        act = conv_silu(jnp.pad(rows, ((CONV_K - 1, 0), (0, 0))), taps, LENGTH)
        xs = act[:, :INNER].reshape(LENGTH, HEADS, HEAD_DIM)
        bm = jnp.repeat(act[:, INNER:INNER + span].reshape(LENGTH, GROUPS, STATE), per_group, axis=1)
        cm = jnp.repeat(act[:, INNER + span:].reshape(LENGTH, GROUPS, STATE), per_group, axis=1)
        step = jax.nn.softplus(s_seq.astype(jnp.float32) + step_bias[None, :])
        y, _ = block_scan(xs, step, rate, bm, cm, BLOCK, jnp.zeros((HEADS, HEAD_DIM, STATE), jnp.float32))
        scanned = (y + skip[None, :, None] * xs).reshape(LENGTH, INNER).astype(jnp.bfloat16)
        gated = (scanned.astype(jnp.float32) * jax.nn.silu(g_seq.astype(jnp.float32))).reshape(LENGTH, GROUPS, INNER // GROUPS)
        gated = gated * lax.rsqrt(lax.optimization_barrier(jnp.mean(gated * gated, axis=2, keepdims=True)) + EPS)
        normed = (gated.reshape(LENGTH, INNER) * norm_gain[None, :]).astype(jnp.bfloat16)
        mixed = (r_seq.astype(jnp.float32) + jnp.dot(normed, out_weight, preferred_element_type=jnp.float32)).astype(jnp.bfloat16)
        mixed_f = mixed.astype(jnp.float32)
        expert_in = (mixed_f * lax.rsqrt(lax.optimization_barrier(jnp.mean(mixed_f * mixed_f, axis=1, keepdims=True)) + EPS) * ffn_gain[None, :]).astype(jnp.bfloat16)
        shared_hidden = (jax.nn.silu(jnp.dot(expert_in, shared_gate, preferred_element_type=jnp.float32)) * jnp.dot(expert_in, shared_up, preferred_element_type=jnp.float32)).astype(jnp.bfloat16)
        base = mixed_f + jnp.dot(shared_hidden, shared_down, preferred_element_type=jnp.float32)
        return (base, expert_in)
    base, expert_in = lax.map(one_sequence, (head_input, b_input, c_input, step_input, gate_input, residual))
    rows_all = SEQS * LENGTH
    flat_in = expert_in.reshape(rows_all, D)
    chosen = routes.reshape(-1).astype(jnp.int32)
    pairs = chosen.shape[0]
    onehot = (chosen[:, None] == jnp.arange(EXPERTS, dtype=jnp.int32)[None, :]).astype(jnp.int32)
    rank = lax.optimization_barrier(jnp.sum((jnp.cumsum(onehot, axis=0) - onehot) * onehot, axis=1)).astype(jnp.int32)
    room = N_SP * N_DP * CAP
    table = jnp.full((EXPERTS, room), pairs, jnp.int32).at[chosen, rank].set(jnp.arange(pairs, dtype=jnp.int32))

    def serve(carry, item):
        index, gate_w, up_w, down_w = item
        rows = jnp.take(flat_in, jnp.minimum(index, pairs - 1) // TOP_K, axis=0)
        hidden = (jax.nn.silu(jnp.dot(rows, gate_w, preferred_element_type=jnp.float32)) * jnp.dot(rows, up_w, preferred_element_type=jnp.float32)).astype(jnp.bfloat16)
        done = jnp.dot(hidden, down_w, preferred_element_type=jnp.float32).astype(jnp.bfloat16)
        return (carry.at[index].set(done, mode='drop'), None)
    pair_out, _ = lax.scan(serve, jnp.zeros((pairs, D), jnp.bfloat16), (table, expert_gate, expert_up, expert_down))
    routed = lax.optimization_barrier(jnp.sum(pair_out.reshape(rows_all, TOP_K, D).astype(jnp.float32) * route_weights.reshape(rows_all, TOP_K, 1), axis=1))
    return (base.reshape(rows_all, D) + routed).astype(jnp.bfloat16).reshape(SEQS, LENGTH, D)
```

```python
import functools

import jax
import jax.numpy as jnp
import numpy as np
from jax import lax
from jax.experimental import pallas as pl
from jax.experimental.pallas import tpu as pltpu
from jax.sharding import PartitionSpec as P

HEAD_DIM = 64
STATE = 128
EPS = 1e-06
HIGH = lax.Precision.HIGHEST
F32 = jnp.float32
BF16 = jnp.bfloat16
EXTRA = 8
MIB = 1 << 20


def dot(a, b, ca, cb, precision=None):
    return lax.dot_general(
        a, b, (((ca,), (cb,)), ((), ())), preferred_element_type=F32, precision=precision
    )


def iota(shape, axis):
    return lax.broadcasted_iota(jnp.int32, shape, axis)


def silu(v):
    return v / (1.0 + jnp.exp(-v))


def vmem(limit):
    return pltpu.CompilerParams(vmem_limit_bytes=limit * MIB)


def cost(flops, nbytes):
    return pl.CostEstimate(flops=flops, bytes_accessed=nbytes, transcendentals=0)


def pack_kernel(width, targets, x_ref, b_ref, c_ref, s_ref, out_ref):
    tokens = x_ref.shape[0]
    ways = out_ref.shape[0]
    local = width // HEAD_DIM
    lanes = out_ref.shape[2]
    eye = (iota((tokens, tokens), 0) == iota((tokens, tokens), 1)).astype(BF16)
    turned = dot(s_ref[...], eye, 0, 0)
    for d in range(ways):
        out_ref[d, 0:tokens, 0:width] = x_ref[:, d * width : (d + 1) * width]
        at = targets[d] * STATE
        out_ref[d, 0:tokens, width : width + STATE] = b_ref[:, at : at + STATE]
        out_ref[d, 0:tokens, width + STATE : width + 2 * STATE] = c_ref[:, at : at + STATE]
        rows = jnp.concatenate(
            [turned[d * local : (d + 1) * local], jnp.zeros((EXTRA - local, tokens), F32)], axis=0
        )
        if tokens < lanes:
            rows = jnp.concatenate([rows, jnp.zeros((EXTRA, lanes - tokens), F32)], axis=1)
        out_ref[d, tokens : tokens + EXTRA, :] = rows.astype(BF16)


def scan_kernel(
    heads, place_ref, got_ref, wx_ref, wb_ref, wc_ref, bias_ref, dlog_ref, skip_ref,
    y_ref, rows_ref, state_ref,
):
    chunks = got_ref.shape[0]
    tokens = got_ref.shape[1] - EXTRA
    width = y_ref.shape[2]
    local = width // HEAD_DIM
    place = place_ref[0]
    rows_ref[0:8] = jnp.zeros((8, rows_ref.shape[1]), F32)
    taps = jnp.concatenate([wx_ref[...], wb_ref[...], wc_ref[...]], axis=1).astype(F32)
    pick = iota((EXTRA, heads), 1) == place * local + iota((EXTRA, heads), 0)
    bias = jnp.sum(jnp.where(pick, bias_ref[...], 0.0), axis=1, keepdims=True)
    rate = -jnp.exp(jnp.sum(jnp.where(pick, dlog_ref[...], 0.0), axis=1, keepdims=True))
    own = iota((heads, width), 0) == place * local + iota((heads, width), 1) // HEAD_DIM
    skip = dot(skip_ref[...], own.astype(F32), 1, 0, HIGH)
    upper = (iota((tokens, tokens), 0) <= iota((tokens, tokens), 1)).astype(F32)
    lower = iota((tokens, tokens), 0) >= iota((tokens, tokens), 1)
    r = iota((2 * EXTRA, 2 * width), 0)
    q = iota((2 * EXTRA, 2 * width), 1)
    spread = (r == (q // width) * EXTRA + (q % width) // HEAD_DIM).astype(F32)
    state_ref[...] = jnp.zeros_like(state_ref)
    for c in range(chunks):
        base = 8 + c * tokens
        rows_ref[base : base + tokens] = got_ref[c, 0:tokens, :].astype(F32)
    for c in range(chunks):
        base = 8 + c * tokens
        act = rows_ref[base : base + tokens] * taps[3:4]
        for k in range(3):
            act = act + rows_ref[pl.ds(base - 3 + k, tokens), :] * taps[k : k + 1]
        act = silu(act)
        xs = act[:, :width]
        bm = act[:, width : width + STATE].astype(BF16)
        cm = act[:, width + STATE :].astype(BF16)
        pre = got_ref[c, tokens : tokens + EXTRA, 0:tokens].astype(F32) + bias
        step = jnp.maximum(pre, 0.0) + jnp.log1p(jnp.exp(-jnp.abs(pre)))
        cum = dot(step * rate, upper, 1, 0, HIGH)
        total = cum[:, tokens - 1 : tokens]
        both = jnp.concatenate([step * jnp.exp(total - cum), jnp.exp(cum - total)], axis=0)
        wide = dot(both, spread, 0, 0, HIGH)
        xw = (xs * wide[:, :width]).astype(BF16)
        scores = jnp.where(lower, dot(cm, bm, 1, 1), 0.0).astype(BF16)
        fade = jnp.exp(total)
        old = jnp.concatenate(
            [
                state_ref[h * HEAD_DIM : (h + 1) * HEAD_DIM, :] * fade[h : h + 1, :]
                for h in range(local)
            ],
            axis=0,
        )
        y = dot(scores, xw, 1, 0) + dot(cm, old.astype(BF16), 1, 1)
        y_ref[c] = (wide[:, width:] * y + skip * xs).astype(BF16)
        if c < chunks - 1:
            state_ref[...] = old + dot(xw, bm, 0, 0)


def slot_of(routes, experts, slots):
    tokens, top = routes.shape
    hot = [iota((tokens, experts), 1) == routes[:, k : k + 1] for k in range(top)]
    count = sum(h.astype(F32) for h in hot).astype(BF16)
    before = (iota((tokens, tokens), 0) > iota((tokens, tokens), 1)).astype(BF16)
    ahead = dot(before, count, 1, 0)
    out = []
    for k in range(top):
        rank = jnp.sum(jnp.where(hot[k], ahead, 0.0), axis=1, keepdims=True)
        out.append(routes[:, k : k + 1] * slots + rank.astype(jnp.int32))
    return out


def mix_kernel(
    blocks, experts, slots, order_ref, got_ref, gate_ref, gain_ref, res_ref, fgain_ref,
    routes_ref, *refs,
):
    count = len(blocks)
    w_refs, (mixed_ref, x_ref, send_ref), (wbuf, acc, sem) = refs[:-6], refs[-6:-3], refs[-3:]
    per = wbuf.shape[1]
    copies = []
    for i, (which, row) in enumerate(blocks):
        copies.append(
            pltpu.make_async_copy(w_refs[which].at[pl.ds(row, per), :], wbuf.at[i], sem.at[i])
        )
        copies[-1].start()
    for i in range(count):
        at = pl.multiple_of(order_ref[i] * per, per)
        sub = got_ref.shape[2]
        if sub == per:
            v = got_ref[order_ref[i]].astype(F32)
        else:
            n = per // sub
            v = jnp.concatenate([got_ref[order_ref[i] * n + k] for k in range(n)], axis=1)
            v = v.astype(F32)
        v = v * silu(gate_ref[:, pl.ds(at, per)].astype(F32))
        v = v * lax.rsqrt(jnp.mean(v * v, axis=1, keepdims=True) + EPS)
        v = (v * gain_ref[:, pl.ds(at, per)]).astype(BF16)
        copies[i].wait()
        part = dot(v, wbuf[i], 1, 0)
        if i == 0:
            acc[...] = part
        else:
            acc[...] += part
    mixed = (res_ref[...].astype(F32) + acc[...]).astype(BF16)
    mixed_ref[...] = mixed
    m = mixed.astype(F32)
    x = m * lax.rsqrt(jnp.mean(m * m, axis=1, keepdims=True) + EPS) * fgain_ref[...]
    x = x.astype(BF16)
    x_ref[...] = x
    tokens = x.shape[0]
    lane = iota((tokens, experts * slots), 1)
    hit = functools.reduce(
        jnp.logical_or, [lane == s for s in slot_of(routes_ref[...], experts, slots)]
    )
    send_ref[...] = dot(hit.astype(BF16), x, 0, 0).astype(BF16)


def shared_kernel(x_ref, mixed_ref, wg_ref, wu_ref, wd_ref, out_ref):
    x = x_ref[...]
    h = (silu(dot(x, wg_ref[...], 1, 0)) * dot(x, wu_ref[...], 1, 0)).astype(BF16)
    out_ref[...] = mixed_ref[...].astype(F32) + dot(h, wd_ref[...], 1, 0)


def expert_kernel(x_ref, wg_ref, wu_ref, wd_ref, out_ref, acc):
    j = pl.program_id(1)
    x = x_ref[...]
    h = (silu(dot(x, wg_ref[0], 1, 0)) * dot(x, wu_ref[0], 1, 0)).astype(BF16)
    part = dot(h, wd_ref[0], 1, 0)

    @pl.when(j == 0)
    def _():
        acc[...] = part

    @pl.when(j > 0)
    def _():
        acc[...] += part

    @pl.when(j == pl.num_programs(1) - 1)
    def _():
        out_ref[...] = acc[...].astype(BF16)


def combine_kernel(experts, slots, got_ref, base_ref, routes_ref, weights_ref, out_ref):
    tokens = base_ref.shape[0]
    lane = iota((tokens, experts * slots), 1)
    w = jnp.zeros((tokens, experts * slots), F32)
    for k, s in enumerate(slot_of(routes_ref[...], experts, slots)):
        w = w + jnp.where(lane == s, weights_ref[:, k : k + 1], 0.0)
    high = w.astype(BF16)
    low = (w - high.astype(F32)).astype(BF16)
    got = got_ref[...]
    out_ref[...] = (base_ref[...] + dot(high, got, 1, 0) + dot(low, got, 1, 0)).astype(BF16)


def gather_rows(w, ways):
    if ways == 4:
        me = lax.axis_index("dp")
        across = lax.ppermute(w, "dp", [(j, j ^ 2) for j in range(4)])
        beside = lax.ppermute(w, "dp", [(j, j ^ 1) for j in range(4)])
        far = lax.ppermute(across, "dp", [(j, j ^ 1) for j in range(4)])
        return [w, beside, across, far], [me, me ^ 1, me ^ 2, me ^ 3]
    return [lax.all_gather(w, "dp", axis=0, tiled=True)], None


def body(
    residual, head_input, gate_input, b_input, c_input, step_input, conv_weight, conv_b_weight,
    conv_c_weight, step_bias, decay_log, skip, norm_gain, out_weight, ffn_gain, shared_gate,
    shared_up, shared_down, expert_gate, expert_up, expert_down, routes, route_weights,
):
    _, tokens, inner = head_input.shape
    features = residual.shape[2]
    heads = step_input.shape[2]
    groups = b_input.shape[2] // STATE
    per_group = heads // groups
    top = routes.shape[2]
    ways = lax.axis_size("sp")
    ways_dp = lax.axis_size("dp")
    experts = ways * ways_dp * expert_gate.shape[0]
    slots = 2 * tokens * top // experts
    place = lax.axis_index("sp").astype(jnp.int32)
    local = heads // ways
    width = local * HEAD_DIM
    targets = [d * local // per_group for d in range(ways)]
    span = inner // groups

    ws, owners = gather_rows(out_weight, ways_dp)
    rows_of = out_weight.shape[0]
    if owners is None:
        blocks = [(0, g * span) for g in range(groups)]
        order = jnp.arange(groups, dtype=jnp.int32)
    else:
        each = rows_of // span
        blocks = [(i, k * span) for i in range(len(ws)) for k in range(each)]
        order = jnp.stack([o * each + k for o in owners for k in range(each)]).astype(jnp.int32)

    lanes = width + 2 * STATE
    packed = pl.pallas_call(
        functools.partial(pack_kernel, width, targets),
        out_shape=jax.ShapeDtypeStruct((ways, tokens + EXTRA, lanes), BF16),
        compiler_params=vmem(16),
        cost_estimate=cost(1 << 20, 4 * MIB),
        name="pack",
    )(head_input[0], b_input[0], c_input[0], step_input[0])
    got = lax.all_to_all(packed, "sp", split_axis=0, concat_axis=0, tiled=True)

    def whole(shape):
        return pl.BlockSpec(shape, lambda i, s: (0,) * len(shape))

    y = pl.pallas_call(
        functools.partial(scan_kernel, heads),
        out_shape=jax.ShapeDtypeStruct((ways, tokens, width), BF16),
        grid_spec=pltpu.PrefetchScalarGridSpec(
            num_scalar_prefetch=1,
            grid=(1,),
            in_specs=[
                whole(got.shape),
                pl.BlockSpec((conv_weight.shape[0], width), lambda i, s: (0, s[0])),
                pl.BlockSpec(
                    (conv_weight.shape[0], STATE), lambda i, s: (0, s[0] * local // per_group)
                ),
                pl.BlockSpec(
                    (conv_weight.shape[0], STATE), lambda i, s: (0, s[0] * local // per_group)
                ),
                whole((1, heads)),
                whole((1, heads)),
                whole((1, heads)),
            ],
            out_specs=whole((ways, tokens, width)),
            scratch_shapes=[
                pltpu.VMEM((8 + ways * tokens, lanes), F32),
                pltpu.VMEM((width, STATE), F32),
            ],
        ),
        compiler_params=vmem(32),
        cost_estimate=cost(1 << 30, 4 * MIB),
        name="scan",
    )(
        place[None], got, conv_weight, conv_b_weight, conv_c_weight,
        step_bias[None], decay_log[None], skip[None],
    )
    back = lax.all_to_all(y, "sp", split_axis=0, concat_axis=0, tiled=True)

    vm = pl.BlockSpec(memory_space=pltpu.VMEM)
    mixed, x, send = pl.pallas_call(
        functools.partial(mix_kernel, blocks, experts, slots),
        out_shape=(
            jax.ShapeDtypeStruct((tokens, features), BF16),
            jax.ShapeDtypeStruct((tokens, features), BF16),
            jax.ShapeDtypeStruct((experts * slots, features), BF16),
        ),
        in_specs=[pl.BlockSpec(memory_space=pltpu.SMEM)]
        + [vm] * 6
        + [pl.BlockSpec(memory_space=pl.ANY)] * len(ws),
        out_specs=(vm, vm, vm),
        scratch_shapes=[
            pltpu.VMEM((groups, span, features), BF16),
            pltpu.VMEM((tokens, features), F32),
            pltpu.SemaphoreType.DMA((groups,)),
        ],
        compiler_params=vmem(48),
        cost_estimate=cost(3 << 30, 16 * MIB),
        name="mix",
    )(
        order, back, gate_input[0], norm_gain[None], residual[0], ffn_gain[None], routes[0], *ws
    )

    base = pl.pallas_call(
        shared_kernel,
        out_shape=jax.ShapeDtypeStruct((tokens, features), F32),
        compiler_params=vmem(32),
        cost_estimate=cost(1 << 30, 8 * MIB),
        name="shared",
    )(x, mixed, shared_gate, shared_up, shared_down)

    arrived = lax.all_to_all(
        send.reshape(experts, slots, features), ("sp", "dp"), split_axis=0, concat_axis=0, tiled=True
    )
    own = expert_gate.shape[0]
    ff = expert_gate.shape[2]
    if own > 1:
        arrived = arrived.reshape(-1, own, slots, features).swapaxes(0, 1)
    arrived = arrived.reshape(own, -1, features)
    m = arrived.shape[1]
    bn = min(256, ff)
    done = pl.pallas_call(
        expert_kernel,
        out_shape=jax.ShapeDtypeStruct((own, m, features), BF16),
        grid=(own, ff // bn),
        in_specs=[
            pl.BlockSpec((None, m, features), lambda e, j: (e, 0, 0)),
            pl.BlockSpec((1, features, bn), lambda e, j: (e, 0, j)),
            pl.BlockSpec((1, features, bn), lambda e, j: (e, 0, j)),
            pl.BlockSpec((1, bn, features), lambda e, j: (e, j, 0)),
        ],
        out_specs=pl.BlockSpec((None, m, features), lambda e, j: (e, 0, 0)),
        scratch_shapes=[pltpu.VMEM((m, features), F32)],
        compiler_params=vmem(48),
        cost_estimate=cost(4 << 30, 10 * MIB),
        name="experts",
    )(arrived, expert_gate, expert_up, expert_down)
    if own > 1:
        done = done.reshape(own, -1, slots, features).swapaxes(0, 1)
    done = done.reshape(experts, slots, features)
    returned = lax.all_to_all(done, ("sp", "dp"), split_axis=0, concat_axis=0, tiled=True)
    out = pl.pallas_call(
        functools.partial(combine_kernel, experts, slots),
        out_shape=jax.ShapeDtypeStruct((tokens, features), BF16),
        compiler_params=vmem(32),
        cost_estimate=cost(1 << 30, 8 * MIB),
        name="combine",
    )(returned.reshape(experts * slots, features), base, routes[0], route_weights[0])
    return out[None]


def solution(mesh):
    tok = P("dp", "sp", None)
    exp = P(("sp", "dp"), None, None)
    return jax.shard_map(
        body,
        mesh=mesh,
        in_specs=(tok,) * 6
        + (P(),) * 7
        + (P("dp", None),)
        + (P(),) * 4
        + (exp,) * 3
        + (tok, tok),
        out_specs=tok,
        check_vma=False,
    )
```

```python
import functools

import jax
import jax.numpy as jnp
from jax import lax
from jax.experimental import pallas as pl
from jax.experimental.pallas import tpu as pltpu
from jax.sharding import PartitionSpec as P


HEAD_DIM = 64
STATE = 128
EPS = 1e-06
HIGH = lax.Precision.HIGHEST
F32 = jnp.float32
BF16 = jnp.bfloat16
EXTRA = 8
TOP = 2
SP = ("half", "sub")
MIB = 1 << 20


def dot(a, b, ca, cb, precision=None):
    return lax.dot_general(
        a, b, (((ca,), (cb,)), ((), ())), preferred_element_type=F32, precision=precision
    )


def iota(shape, axis):
    return lax.broadcasted_iota(jnp.int32, shape, axis)


def silu(v):
    return v / (1.0 + jnp.exp(-v))


def vmem(limit):
    return pltpu.CompilerParams(vmem_limit_bytes=limit * MIB)


def cost(flops, nbytes):
    return pl.CostEstimate(flops=flops, bytes_accessed=nbytes, transcendentals=0)


def tail_kernel(x_ref, b_ref, c_ref, out_ref, sem):
    copies = []
    start = 0
    rows = out_ref.shape[0]
    for i, ref in enumerate((x_ref, b_ref, c_ref)):
        size = ref.shape[1]
        copies.append(
            pltpu.make_async_copy(
                ref.at[pl.ds(ref.shape[0] - rows, rows), :],
                out_ref.at[:, pl.ds(start, size)],
                sem.at[i],
            )
        )
        copies[-1].start()
        start += size
    for copy in copies:
        copy.wait()


def conv_silu(rows_in, tail, taps, rows_ref):
    tokens = rows_in.shape[0]
    rows_ref[0:8] = tail.astype(F32)
    rows_ref[8 : 8 + tokens] = rows_in.astype(F32)
    taps = taps.astype(F32)
    act = rows_ref[8 : 8 + tokens] * taps[3:4]
    for k in range(3):
        act = act + rows_ref[5 + k : 5 + k + tokens] * taps[k : k + 1]
    return silu(act)


def decays(s_ref, bias_ref, dlog_ref):
    heads, tokens = s_ref.shape
    same = iota((heads, heads), 0) == iota((heads, heads), 1)
    bias, dlog = (
        jnp.sum(jnp.where(same, ref[...], 0.0), axis=1, keepdims=True)
        for ref in (bias_ref, dlog_ref)
    )
    pre = s_ref[...].astype(F32) + bias
    step = jnp.maximum(pre, 0.0) + jnp.log1p(jnp.exp(-jnp.abs(pre)))
    upper = (iota((tokens, tokens), 0) <= iota((tokens, tokens), 1)).astype(F32)
    cum = dot(step * -jnp.exp(dlog), upper, 1, 0, HIGH)
    return step, cum, cum[:, tokens - 1 : tokens]


def spread(v, inner):
    heads = v.shape[0]
    a = v.astype(BF16)
    rest = v - a.astype(F32)
    b = rest.astype(BF16)
    c = (rest - b.astype(F32)).astype(BF16)
    own = (iota((heads, inner), 0) == iota((heads, inner), 1) // HEAD_DIM).astype(BF16)
    return dot(jnp.concatenate([a, b, c], axis=0), jnp.concatenate([own] * 3, axis=0), 0, 0)


def state_kernel(
    s_ref, bias_ref, dlog_ref, tail_ref, wx_ref, wb_ref, x_ref, b_ref, out_ref, rx_ref, rb_ref
):
    inner = x_ref.shape[1]
    ways = out_ref.shape[0]
    rows = out_ref.shape[1] - EXTRA
    local = rows // HEAD_DIM
    span = inner // (b_ref.shape[1] // STATE)
    step, cum, total = decays(s_ref, bias_ref, dlog_ref)
    wide = spread(step * jnp.exp(total - cum), inner)
    fade = jnp.exp(jnp.broadcast_to(total, (total.shape[0], STATE)))
    high = fade.astype(BF16).astype(F32)
    low = fade - high
    bm = conv_silu(b_ref[...], tail_ref[:, inner : inner + b_ref.shape[1]], wb_ref[...], rb_ref)
    bm = bm.astype(BF16)
    xs = conv_silu(x_ref[...], tail_ref[:, :inner], wx_ref[...], rx_ref)
    xw = (xs * wide).astype(BF16)
    blank = jnp.zeros((EXTRA // 2 - local, STATE), F32)
    for d in range(ways):
        g = d * rows // span
        st = dot(xw[:, d * rows : (d + 1) * rows], bm[:, g * STATE : (g + 1) * STATE], 0, 0)
        out_ref[d, 0:rows, :] = st.astype(BF16)
        own = slice(d * local, (d + 1) * local)
        parts = [high[own], low[own]]
        if local < EXTRA // 2:
            parts = [high[own], blank, low[own], blank]
        out_ref[d, rows : rows + EXTRA, :] = jnp.concatenate(parts, axis=0).astype(BF16)


def prefix_kernel(in_hbm, out_hbm, in_ref, out_ref, sem_in, sem_out):
    ways, rows, _ = out_ref.shape
    gets = [pltpu.make_async_copy(in_hbm.at[j], in_ref.at[j], sem_in.at[j]) for j in range(ways)]
    puts = [pltpu.make_async_copy(out_ref.at[j], out_hbm.at[j], sem_out.at[j]) for j in range(ways)]
    for get in gets:
        get.start()
    state = jnp.zeros((rows, STATE), F32)
    for j in range(ways):
        gets[j].wait()
        fade = in_ref[j, rows : rows + EXTRA, :].astype(F32)
        old = jnp.concatenate(
            [
                state[h * HEAD_DIM : (h + 1) * HEAD_DIM]
                * (fade[h : h + 1] + fade[h + EXTRA // 2 : h + 1 + EXTRA // 2])
                for h in range(rows // HEAD_DIM)
            ],
            axis=0,
        )
        out_ref[j] = old.astype(BF16)
        puts[j].start()
        state = old + in_ref[j, 0:rows, :].astype(F32)
    for put in puts:
        put.wait()


def inner_kernel(
    s_ref, bias_ref, dlog_ref, skip_ref, tail_ref, wx_ref, wb_ref, wc_ref, x_ref, b_ref, c_ref,
    y_ref, grow_ref, cm_ref, rx_ref, rb_ref,
):
    tokens, inner = x_ref.shape
    heads = s_ref.shape[0]
    narrow = b_ref.shape[1]
    groups = narrow // STATE
    span = inner // groups
    step, cum, total = decays(s_ref, bias_ref, dlog_ref)
    wide = spread(step * jnp.exp(total - cum), inner)
    grow = spread(jnp.exp(cum - total), inner)
    grow_ref[...] = grow
    own = (iota((heads, inner), 0) == iota((heads, inner), 1) // HEAD_DIM).astype(F32)
    skip = dot(skip_ref[...], own, 1, 0, HIGH)
    bm = conv_silu(b_ref[...], tail_ref[:, inner : inner + narrow], wb_ref[...], rb_ref)
    bm = bm.astype(BF16)
    cm = conv_silu(c_ref[...], tail_ref[:, inner + narrow :], wc_ref[...], rb_ref).astype(BF16)
    cm_ref[...] = cm
    xs = conv_silu(x_ref[...], tail_ref[:, :inner], wx_ref[...], rx_ref)
    xw = (xs * wide).astype(BF16)
    lower = iota((tokens, tokens), 0) >= iota((tokens, tokens), 1)
    for g in range(groups):
        n = slice(g * STATE, (g + 1) * STATE)
        at = slice(g * span, (g + 1) * span)
        scores = jnp.where(lower, dot(cm[:, n], bm[:, n], 1, 1), 0.0).astype(BF16)
        y_ref[:, at] = grow[:, at] * dot(scores, xw[:, at], 1, 0) + skip[:, at] * xs[:, at]


def slot_of(meta, experts, slots):
    tokens = meta.shape[1]
    top = TOP
    same = (iota((tokens, tokens), 0) == iota((tokens, tokens), 1)).astype(F32)
    cols = dot(same, meta, 1, 1, HIGH)
    lane = iota((tokens, experts), 1).astype(F32)
    hot = [lane == cols[:, k : k + 1] for k in range(top)]
    count = sum(h.astype(F32) for h in hot).astype(BF16)
    before = (iota((tokens, tokens), 0) > iota((tokens, tokens), 1)).astype(BF16)
    ahead = dot(before, count, 1, 0)
    out = []
    for k in range(top):
        rank = jnp.sum(jnp.where(hot[k], ahead, 0.0), axis=1, keepdims=True)
        out.append((cols[:, k : k + 1] * slots + rank, cols[:, top + k : top + k + 1]))
    return out


def hits(meta, experts, slots, half, rows):
    lane = (iota((meta.shape[1], rows), 1) + half * rows).astype(F32)
    found = [lane == s for s, _ in slot_of(meta, experts, slots)]
    return functools.reduce(jnp.logical_or, found).astype(BF16)


def weighted(meta, experts, slots, half, got):
    lane = (iota((meta.shape[1], got.shape[0]), 1) + half * got.shape[0]).astype(F32)
    w = jnp.zeros(lane.shape, F32)
    for s, value in slot_of(meta, experts, slots):
        w = w + jnp.where(lane == s, value, 0.0)
    high = w.astype(BF16)
    low = (w - high.astype(F32)).astype(BF16)
    return dot(high, got, 1, 0) + dot(low, got, 1, 0)


def mix_kernel(
    blocks, experts, slots, order_ref, gain_ref, fgain_ref, meta_ref, state_in, y_in, grow_in,
    cm_in, gate_in, res_in, *refs,
):
    count = len(blocks)
    w_refs, (mixed_ref, x_ref, send_ref) = refs[:-19], refs[-19:-16]
    wbuf, state_ref, y_ref, grow_ref, cm_ref, gate_ref, res_ref = refs[-16:-9]
    acc, mbuf, xbuf, sbuf, sem_w, sem_v, sem_m, sem_x, sem_s = refs[-9:]
    per = wbuf.shape[1]
    odd = order_ref[count + 1]
    copies = []
    for i, pieces in enumerate(blocks):
        at = pl.multiple_of(order_ref[i] * per, per)
        col = pl.multiple_of(order_ref[i] * STATE, STATE)
        wide = pl.ds(at, per)
        pairs = [
            (state_in.at[wide, :], state_ref.at[i]),
            (cm_in.at[:, pl.ds(col, STATE)], cm_ref.at[i]),
            (y_in.at[:, wide], y_ref.at[i]),
            (grow_in.at[:, wide], grow_ref.at[i]),
            (gate_in.at[:, wide], gate_ref.at[i]),
        ]
        small = [pltpu.make_async_copy(a, b, sem_v.at[i, k]) for k, (a, b) in enumerate(pairs)]
        large = []
        for k, (which, row, size, side) in enumerate(pieces):
            if side is None:
                to = pl.ds(0, size)
            else:
                to = pl.ds(pl.multiple_of((odd if side == 0 else 1 - odd) * size, size), size)
            large.append(
                pltpu.make_async_copy(
                    w_refs[which].at[pl.ds(row, size), :], wbuf.at[i, to], sem_w.at[i, k]
                )
            )
        for copy in small + large:
            copy.start()
        copies.append((small, large))
    residual = pltpu.make_async_copy(res_in, res_ref, sem_v.at[count, 0])
    residual.start()
    for i in range(count):
        at = pl.multiple_of(order_ref[i] * per, per)
        for copy in copies[i][0]:
            copy.wait()
        v = y_ref[i] + grow_ref[i] * dot(cm_ref[i], state_ref[i], 1, 1)
        v = v.astype(BF16).astype(F32)
        v = v * silu(gate_ref[i].astype(F32))
        v = v * lax.rsqrt(jnp.mean(v * v, axis=1, keepdims=True) + EPS)
        v = (v * gain_ref[:, pl.ds(at, per)]).astype(BF16)
        for copy in copies[i][1]:
            copy.wait()
        part = dot(v, wbuf[i], 1, 0)
        if i == 0:
            acc[...] = part
        else:
            acc[...] += part
    residual.wait()
    mixed = (res_ref[...].astype(F32) + acc[...]).astype(BF16)
    mbuf[...] = mixed
    out_mixed = pltpu.make_async_copy(mbuf, mixed_ref, sem_m)
    out_mixed.start()
    m = mixed.astype(F32)
    x = m * lax.rsqrt(jnp.mean(m * m, axis=1, keepdims=True) + EPS) * fgain_ref[...]
    x = x.astype(BF16)
    xbuf[...] = x
    out_x = pltpu.make_async_copy(xbuf, x_ref, sem_x)
    out_x.start()
    place_rows(
        hits(meta_ref[...], experts, slots, order_ref[count], send_ref.shape[0]),
        x, sbuf, send_ref, sem_s,
    )
    out_x.wait()
    out_mixed.wait()


def place_rows(hit, x, sbuf, send_ref, sem):
    pieces = sem.shape[0]
    rows = send_ref.shape[0] // pieces
    copies = []
    for i in range(pieces):
        part = slice(i * rows, (i + 1) * rows)
        sbuf[part] = dot(hit[:, part], x, 0, 0).astype(BF16)
        copies.append(
            pltpu.make_async_copy(
                sbuf.at[pl.ds(i * rows, rows)], send_ref.at[pl.ds(i * rows, rows)], sem.at[i]
            )
        )
        copies[-1].start()
    for copy in copies:
        copy.wait()


def relay_kernel(experts, slots, half_ref, meta_ref, x_in, send_ref, x_ref, sbuf, sem_x, sem):
    copy = pltpu.make_async_copy(x_in, x_ref, sem_x)
    copy.start()
    hit = hits(meta_ref[...], experts, slots, half_ref[0], send_ref.shape[0])
    copy.wait()
    place_rows(hit, x_ref[...], sbuf, send_ref, sem)


def shared_kernel(x_in, mixed_in, wg_in, wu_in, wd_in, out_ref, x_ref, m_ref, wg, wu, wd, sem):
    copies = [
        pltpu.make_async_copy(src, dst, sem.at[i])
        for i, (src, dst) in enumerate(
            ((x_in, x_ref), (wg_in, wg), (wu_in, wu), (wd_in, wd), (mixed_in, m_ref))
        )
    ]
    for copy in copies:
        copy.start()
    for copy in copies[:3]:
        copy.wait()
    x = x_ref[...]
    h = (silu(dot(x, wg[...], 1, 0)) * dot(x, wu[...], 1, 0)).astype(BF16)
    for copy in copies[3:]:
        copy.wait()
    out_ref[...] = m_ref[...].astype(F32) + dot(h, wd[...], 1, 0)


def expert_kernel(x_ref, wg_ref, wu_ref, wd_ref, out_ref, acc, obuf, sem):
    e = pl.program_id(0)
    j = pl.program_id(1)
    x = x_ref[...]
    h = (silu(dot(x, wg_ref[0], 1, 0)) * dot(x, wu_ref[0], 1, 0)).astype(BF16)
    part = dot(h, wd_ref[0], 1, 0)

    @pl.when(j == 0)
    def _():
        acc[...] = part

    @pl.when(j == pl.num_programs(1) - 1)
    def _():
        pieces = sem.shape[0]
        rows = obuf.shape[0] // pieces
        copies = []
        for i in range(pieces):
            at = slice(i * rows, (i + 1) * rows)
            obuf[at] = (acc[at] + part[at]).astype(BF16)
            copies.append(
                pltpu.make_async_copy(
                    obuf.at[pl.ds(i * rows, rows)], out_ref.at[e, pl.ds(i * rows, rows)], sem.at[i]
                )
            )
            copies[-1].start()
        for copy in copies:
            copy.wait()


def part_kernel(experts, slots, half_ref, meta_ref, got_ref, out_ref, obuf, sem):
    obuf[...] = weighted(meta_ref[...], experts, slots, half_ref[0], got_ref[...]).astype(BF16)
    copy = pltpu.make_async_copy(obuf, out_ref, sem)
    copy.start()
    copy.wait()


def combine_kernel(experts, slots, half_ref, meta_ref, got_ref, base_ref, other_ref, out_ref):
    own = weighted(meta_ref[...], experts, slots, half_ref[0], got_ref[...])
    out_ref[...] = (base_ref[...] + own + other_ref[...].astype(F32)).astype(BF16)


def gather_rows(w, ways, span):
    if ways == 4 and w.shape[0] == 2 * span and lax.axis_size("sub") % 2 == 0:
        me = lax.axis_index("dp")
        odd = lax.rem(lax.axis_index("sub"), 2).astype(jnp.int32)
        part = span // 2
        over = [(j, j ^ 2) for j in range(4)]
        core = [(j, j ^ 1) for j in range(4)]
        flip = [(j, j ^ 1) for j in range(lax.axis_size("sub"))]
        xa = lax.ppermute(lax.dynamic_slice_in_dim(w, odd * part, part, 0), "dp", over)
        xb = lax.ppermute(w[span:], "dp", over)
        ya = lax.ppermute(xa, "sub", flip)
        beside = lax.ppermute(w, "dp", core)
        fa = lax.ppermute(xa, "dp", core)
        fy = lax.ppermute(ya, "dp", core)
        fb = lax.ppermute(xb, "dp", core)
        arrays = [w, beside, xa, ya, xb, fa, fy, fb]
        blocks = [[(i, k * span, span, None)] for i in range(2) for k in range(2)]
        for i in (2, 5):
            blocks.append([(i, 0, part, 0), (i + 1, 0, part, 1)])
            blocks.append([(i + 2, 0, span, None)])
        order = [(me ^ i) * 2 + k for i in range(4) for k in range(2)]
        return arrays, blocks, order, odd
    whole = lax.all_gather(w, "dp", axis=0, tiled=True)
    count = whole.shape[0] // span
    blocks = [[(0, g * span, span, None)] for g in range(count)]
    return [whole], blocks, list(range(count)), jnp.int32(0)


def layer(
    residual, head_input, gate_input, b_input, c_input, step_input, conv_weight, conv_b_weight,
    conv_c_weight, step_bias, decay_log, skip, norm_gain, out_weight, ffn_gain, shared_gate,
    shared_up, shared_down, expert_gate, expert_up, expert_down, routes, route_weights,
):
    _, tokens, inner = head_input.shape
    features = residual.shape[2]
    heads = step_input.shape[2]
    groups = b_input.shape[2] // STATE
    top = routes.shape[2]
    ways = lax.axis_size(SP)
    ways_dp = lax.axis_size("dp")
    experts = ways * ways_dp * expert_gate.shape[0]
    slots = 2 * tokens * top // experts
    local = heads // ways
    width = local * HEAD_DIM
    span = inner // groups

    ws, blocks, order, odd = gather_rows(out_weight, ways_dp, span)
    half = lax.axis_index("half").astype(jnp.int32)
    order = jnp.stack([jnp.asarray(o, jnp.int32) for o in order + [half, odd]])
    meta = jnp.concatenate([routes[0].T.astype(F32), route_weights[0].T], axis=0)
    meta = jnp.concatenate([meta, jnp.zeros((8 - 2 * top, tokens), F32)], axis=0)
    mirror = [(0, 1), (1, 0)]
    meta_far = lax.ppermute(meta, "half", mirror)
    rows = experts * slots // 2
    pieces = 4

    hbm = pl.BlockSpec(memory_space=pltpu.HBM)
    vm = pl.BlockSpec(memory_space=pltpu.VMEM)
    x_in, b_in, c_in = head_input[0], b_input[0], c_input[0]
    turned = (step_input[0].T, step_bias[None], decay_log[None])
    tail = pl.pallas_call(
        tail_kernel,
        out_shape=jax.ShapeDtypeStruct((8, inner + 2 * b_in.shape[1]), BF16),
        in_specs=[hbm] * 3,
        out_specs=vm,
        scratch_shapes=[pltpu.SemaphoreType.DMA((3,))],
        compiler_params=vmem(60),
        cost_estimate=cost(1 << 10, 1 << 17),
        name="tails",
    )(x_in, b_in, c_in)
    tail = lax.ppermute(tail, SP, [(i, i + 1) for i in range(ways - 1)])
    fresh = pl.pallas_call(
        state_kernel,
        out_shape=jax.ShapeDtypeStruct((ways, width + EXTRA, STATE), BF16),
        in_specs=[vm] * 8,
        out_specs=vm,
        scratch_shapes=[
            pltpu.VMEM((8 + tokens, inner), F32),
            pltpu.VMEM((8 + tokens, b_in.shape[1]), F32),
        ],
        compiler_params=vmem(60),
        cost_estimate=cost(1 << 30, 4 * MIB),
        name="states",
    )(*turned, tail, conv_weight, conv_b_weight, x_in, b_in)
    fresh = lax.all_to_all(fresh, SP, split_axis=0, concat_axis=0, tiled=True)
    y, grow, cm = pl.pallas_call(
        inner_kernel,
        out_shape=(
            jax.ShapeDtypeStruct((tokens, inner), F32),
            jax.ShapeDtypeStruct((tokens, inner), F32),
            jax.ShapeDtypeStruct((tokens, b_in.shape[1]), BF16),
        ),
        in_specs=[vm] * 11,
        out_specs=(vm,) * 3,
        scratch_shapes=[
            pltpu.VMEM((8 + tokens, inner), F32),
            pltpu.VMEM((8 + tokens, b_in.shape[1]), F32),
        ],
        compiler_params=vmem(60),
        cost_estimate=cost(2 << 30, 8 * MIB),
        name="within",
    )(
        *turned, skip[None], tail, conv_weight, conv_b_weight, conv_c_weight, x_in, b_in, c_in
    )
    entering = pl.pallas_call(
        prefix_kernel,
        out_shape=jax.ShapeDtypeStruct((ways, width, STATE), BF16),
        in_specs=[hbm],
        out_specs=hbm,
        scratch_shapes=[
            pltpu.VMEM(fresh.shape, BF16),
            pltpu.VMEM((ways, width, STATE), BF16),
            pltpu.SemaphoreType.DMA((ways,)),
            pltpu.SemaphoreType.DMA((ways,)),
        ],
        compiler_params=vmem(60),
        cost_estimate=cost(1 << 26, 2 * MIB),
        name="prefix",
    )(fresh)
    entering = lax.all_to_all(entering, SP, split_axis=0, concat_axis=0, tiled=True)
    entering = entering.reshape(inner, STATE)

    sm = pl.BlockSpec(memory_space=pltpu.SMEM)
    mixed, x, send = pl.pallas_call(
        functools.partial(mix_kernel, blocks, experts, slots),
        out_shape=(
            jax.ShapeDtypeStruct((tokens, features), BF16),
            jax.ShapeDtypeStruct((tokens, features), BF16),
            jax.ShapeDtypeStruct((rows, features), BF16),
        ),
        in_specs=[sm] + [vm] * 3 + [hbm] * (6 + len(ws)),
        out_specs=(hbm, hbm, hbm),
        scratch_shapes=[
            pltpu.VMEM((groups, span, features), BF16),
            pltpu.VMEM((groups, span, STATE), BF16),
            pltpu.VMEM((groups, tokens, span), F32),
            pltpu.VMEM((groups, tokens, span), F32),
            pltpu.VMEM((groups, tokens, STATE), BF16),
            pltpu.VMEM((groups, tokens, span), BF16),
            pltpu.VMEM((tokens, features), BF16),
            pltpu.VMEM((tokens, features), F32),
            pltpu.VMEM((tokens, features), BF16),
            pltpu.VMEM((tokens, features), BF16),
            pltpu.VMEM((rows, features), BF16),
            pltpu.SemaphoreType.DMA((groups, 2)),
            pltpu.SemaphoreType.DMA((groups + 1, 5)),
            pltpu.SemaphoreType.DMA,
            pltpu.SemaphoreType.DMA,
            pltpu.SemaphoreType.DMA((pieces,)),
        ],
        compiler_params=vmem(62),
        cost_estimate=cost(3 << 30, 16 * MIB),
        name="mix",
    )(
        order, norm_gain[None], ffn_gain[None], meta, entering, y, grow, cm, gate_input[0],
        residual[0], *ws,
    )

    x_far = lax.ppermute(x, "half", mirror)
    group = ("sub", "dp")

    def exchange(v):
        v = v.reshape(-1, slots, features)
        return lax.all_to_all(v, group, split_axis=0, concat_axis=0, tiled=True)

    own = expert_gate.shape[0]
    ff = expert_gate.shape[2]
    bn = ff // 2

    def serve(arrived):
        if own > 1:
            arrived = arrived.reshape(-1, own, slots, features).swapaxes(0, 1)
        arrived = arrived.reshape(own, -1, features)
        m = arrived.shape[1]
        done = pl.pallas_call(
            expert_kernel,
            out_shape=jax.ShapeDtypeStruct((own, m, features), BF16),
            grid=(own, ff // bn),
            in_specs=[
                pl.BlockSpec((None, m, features), lambda e, j: (e, 0, 0)),
                pl.BlockSpec((1, features, bn), lambda e, j: (e, 0, j)),
                pl.BlockSpec((1, features, bn), lambda e, j: (e, 0, j)),
                pl.BlockSpec((1, bn, features), lambda e, j: (e, j, 0)),
            ],
            out_specs=hbm,
            scratch_shapes=[
                pltpu.VMEM((m, features), F32),
                pltpu.VMEM((m, features), BF16),
                pltpu.SemaphoreType.DMA((pieces,)),
            ],
            compiler_params=vmem(48),
            cost_estimate=cost(2 << 30, 8 * MIB),
            name="experts",
        )(arrived, expert_gate, expert_up, expert_down)
        if own > 1:
            done = done.reshape(own, -1, slots, features).swapaxes(0, 1)
        return done

    near = exchange(send)
    base = pl.pallas_call(
        shared_kernel,
        out_shape=jax.ShapeDtypeStruct((tokens, features), F32),
        in_specs=[hbm] * 5,
        out_specs=vm,
        scratch_shapes=[
            pltpu.VMEM(v.shape, BF16) for v in (x, mixed, shared_gate, shared_up, shared_down)
        ]
        + [pltpu.SemaphoreType.DMA((5,))],
        compiler_params=vmem(62),
        cost_estimate=cost(1 << 30, 8 * MIB),
        name="shared",
    )(x, mixed, shared_gate, shared_up, shared_down)
    near = serve(near)
    relay = pl.pallas_call(
        functools.partial(relay_kernel, experts, slots),
        out_shape=jax.ShapeDtypeStruct((rows, features), BF16),
        in_specs=[sm, vm, hbm],
        out_specs=hbm,
        scratch_shapes=[
            pltpu.VMEM((tokens, features), BF16),
            pltpu.VMEM((rows, features), BF16),
            pltpu.SemaphoreType.DMA,
            pltpu.SemaphoreType.DMA((pieces,)),
        ],
        compiler_params=vmem(32),
        cost_estimate=cost(1 << 28, 3 * MIB),
        name="relay",
    )(half[None], meta_far, x_far)
    far = exchange(relay)
    far = serve(far)
    far = exchange(far)
    part = pl.pallas_call(
        functools.partial(part_kernel, experts, slots),
        out_shape=jax.ShapeDtypeStruct((tokens, features), BF16),
        in_specs=[sm, vm, vm],
        out_specs=hbm,
        scratch_shapes=[pltpu.VMEM((tokens, features), BF16), pltpu.SemaphoreType.DMA],
        compiler_params=vmem(32),
        cost_estimate=cost(1 << 29, 3 * MIB),
        name="part",
    )(half[None], meta_far, far.reshape(rows, features))
    other = lax.ppermute(part, "half", mirror)
    near = exchange(near)
    out = pl.pallas_call(
        functools.partial(combine_kernel, experts, slots),
        out_shape=jax.ShapeDtypeStruct((tokens, features), BF16),
        in_specs=[sm] + [vm] * 4,
        out_specs=vm,
        compiler_params=vmem(32),
        cost_estimate=cost(1 << 29, 4 * MIB),
        name="combine",
    )(half[None], meta, near.reshape(rows, features), base, other)
    return out[None]


def solution(mesh):
    ways, ways_dp = mesh.devices.shape
    mesh = jax.sharding.Mesh(mesh.devices.reshape(2, ways // 2, ways_dp), SP + ("dp",))
    tok = P("dp", SP, None)
    exp = P(SP + ("dp",), None, None)
    return jax.shard_map(
        layer,
        mesh=mesh,
        in_specs=(tok,) * 6
        + (P(),) * 7
        + (P("dp", None),)
        + (P(),) * 4
        + (exp,) * 3
        + (tok, tok),
        out_specs=tok,
        check_vma=False,
    )
```

```python
import functools

import jax
import jax.numpy as jnp
from jax import lax
from jax.experimental import pallas as pl
from jax.experimental.pallas import tpu as pltpu
from jax.sharding import PartitionSpec as P


HEAD_DIM = 64
STATE = 128
EPS = 1e-06
HIGH = lax.Precision.HIGHEST
F32 = jnp.float32
BF16 = jnp.bfloat16
EXTRA = 8
TOP = 2
SP = ("half", "sub")
MIB = 1 << 20


def dot(a, b, ca, cb, precision=None):
    return lax.dot_general(
        a, b, (((ca,), (cb,)), ((), ())), preferred_element_type=F32, precision=precision
    )


def iota(shape, axis):
    return lax.broadcasted_iota(jnp.int32, shape, axis)


def silu(v):
    return v / (1.0 + jnp.exp(-v))


def vmem(limit):
    return pltpu.CompilerParams(vmem_limit_bytes=limit * MIB)


def inside(v):
    return pltpu.with_memory_space_constraint(v, pltpu.VMEM)


def outside(v):
    return pltpu.with_memory_space_constraint(v, pltpu.HBM)


def cost(flops, nbytes):
    return pl.CostEstimate(flops=flops, bytes_accessed=nbytes, transcendentals=0)


def tail_kernel(x_ref, b_ref, c_ref, out_ref, sem):
    copies = []
    start = 0
    rows = out_ref.shape[0]
    for i, ref in enumerate((x_ref, b_ref, c_ref)):
        size = ref.shape[1]
        copies.append(
            pltpu.make_async_copy(
                ref.at[pl.ds(ref.shape[0] - rows, rows), :],
                out_ref.at[:, pl.ds(start, size)],
                sem.at[i],
            )
        )
        copies[-1].start()
        start += size
    for copy in copies:
        copy.wait()


def conv_silu(rows_in, tail, taps, rows_ref):
    tokens = rows_in.shape[0]
    rows_ref[0:8] = tail.astype(F32)
    rows_ref[8 : 8 + tokens] = rows_in.astype(F32)
    taps = taps.astype(F32)
    act = rows_ref[8 : 8 + tokens] * taps[3:4]
    for k in range(3):
        act = act + rows_ref[5 + k : 5 + k + tokens] * taps[k : k + 1]
    return silu(act)


def decays(s_ref, bias_ref, dlog_ref):
    heads, tokens = s_ref.shape
    same = iota((heads, heads), 0) == iota((heads, heads), 1)
    bias, dlog = (
        jnp.sum(jnp.where(same, ref[...], 0.0), axis=1, keepdims=True)
        for ref in (bias_ref, dlog_ref)
    )
    pre = s_ref[...].astype(F32) + bias
    step = jnp.maximum(pre, 0.0) + jnp.log1p(jnp.exp(-jnp.abs(pre)))
    upper = (iota((tokens, tokens), 0) <= iota((tokens, tokens), 1)).astype(F32)
    cum = dot(step * -jnp.exp(dlog), upper, 1, 0, HIGH)
    return step, cum, cum[:, tokens - 1 : tokens]


def spread(v, inner):
    heads = v.shape[0]
    a = v.astype(BF16)
    rest = v - a.astype(F32)
    b = rest.astype(BF16)
    c = (rest - b.astype(F32)).astype(BF16)
    own = (iota((heads, inner), 0) == iota((heads, inner), 1) // HEAD_DIM).astype(BF16)
    return dot(jnp.concatenate([a, b, c], axis=0), jnp.concatenate([own] * 3, axis=0), 0, 0)


def state_kernel(
    s_ref, bias_ref, dlog_ref, tail_ref, wx_ref, wb_ref, x_ref, b_ref, out_ref, rx_ref, rb_ref
):
    inner = x_ref.shape[1]
    ways = out_ref.shape[0]
    rows = out_ref.shape[1] - EXTRA
    local = rows // HEAD_DIM
    span = inner // (b_ref.shape[1] // STATE)
    step, cum, total = decays(s_ref, bias_ref, dlog_ref)
    wide = spread(step * jnp.exp(total - cum), inner)
    fade = jnp.exp(jnp.broadcast_to(total, (total.shape[0], STATE)))
    high = fade.astype(BF16).astype(F32)
    low = fade - high
    bm = conv_silu(b_ref[...], tail_ref[:, inner : inner + b_ref.shape[1]], wb_ref[...], rb_ref)
    bm = bm.astype(BF16)
    xs = conv_silu(x_ref[...], tail_ref[:, :inner], wx_ref[...], rx_ref)
    xw = (xs * wide).astype(BF16)
    blank = jnp.zeros((EXTRA // 2 - local, STATE), F32)
    for d in range(ways):
        g = d * rows // span
        st = dot(xw[:, d * rows : (d + 1) * rows], bm[:, g * STATE : (g + 1) * STATE], 0, 0)
        out_ref[d, 0:rows, :] = st.astype(BF16)
        own = slice(d * local, (d + 1) * local)
        parts = [high[own], low[own]]
        if local < EXTRA // 2:
            parts = [high[own], blank, low[own], blank]
        out_ref[d, rows : rows + EXTRA, :] = jnp.concatenate(parts, axis=0).astype(BF16)


def prefix_kernel(in_ref, out_hbm, out_ref, sem_out):
    ways, rows, _ = out_ref.shape
    puts = [pltpu.make_async_copy(out_ref.at[j], out_hbm.at[j], sem_out.at[j]) for j in range(ways)]
    state = jnp.zeros((rows, STATE), F32)
    for j in range(ways):
        fade = in_ref[j, rows : rows + EXTRA, :].astype(F32)
        old = jnp.concatenate(
            [
                state[h * HEAD_DIM : (h + 1) * HEAD_DIM]
                * (fade[h : h + 1] + fade[h + EXTRA // 2 : h + 1 + EXTRA // 2])
                for h in range(rows // HEAD_DIM)
            ],
            axis=0,
        )
        out_ref[j] = old.astype(BF16)
        puts[j].start()
        state = old + in_ref[j, 0:rows, :].astype(F32)
    for put in puts:
        put.wait()


def inner_kernel(
    s_ref, bias_ref, dlog_ref, skip_ref, tail_ref, wx_ref, wb_ref, wc_ref, x_ref, b_ref, c_ref,
    y_ref, grow_ref, cm_ref, rx_ref, rb_ref,
):
    tokens, inner = x_ref.shape
    heads = s_ref.shape[0]
    narrow = b_ref.shape[1]
    groups = narrow // STATE
    span = inner // groups
    step, cum, total = decays(s_ref, bias_ref, dlog_ref)
    wide = spread(step * jnp.exp(total - cum), inner)
    grow_ref[...] = jnp.exp(cum - total)
    grow = spread(grow_ref[...], inner)
    own = (iota((heads, inner), 0) == iota((heads, inner), 1) // HEAD_DIM).astype(F32)
    skip = dot(skip_ref[...], own, 1, 0, HIGH)
    bm = conv_silu(b_ref[...], tail_ref[:, inner : inner + narrow], wb_ref[...], rb_ref)
    bm = bm.astype(BF16)
    cm = conv_silu(c_ref[...], tail_ref[:, inner + narrow :], wc_ref[...], rb_ref).astype(BF16)
    cm_ref[...] = cm
    xs = conv_silu(x_ref[...], tail_ref[:, :inner], wx_ref[...], rx_ref)
    xw = (xs * wide).astype(BF16)
    lower = iota((tokens, tokens), 0) >= iota((tokens, tokens), 1)
    for g in range(groups):
        n = slice(g * STATE, (g + 1) * STATE)
        at = slice(g * span, (g + 1) * span)
        scores = jnp.where(lower, dot(cm[:, n], bm[:, n], 1, 1), 0.0).astype(BF16)
        y_ref[:, at] = grow[:, at] * dot(scores, xw[:, at], 1, 0) + skip[:, at] * xs[:, at]


def slot_of(meta, experts, slots):
    tokens = meta.shape[1]
    top = TOP
    same = (iota((tokens, tokens), 0) == iota((tokens, tokens), 1)).astype(F32)
    cols = dot(same, meta, 1, 1, HIGH)
    lane = iota((tokens, experts), 1).astype(F32)
    hot = [lane == cols[:, k : k + 1] for k in range(top)]
    count = sum(h.astype(F32) for h in hot).astype(BF16)
    before = (iota((tokens, tokens), 0) > iota((tokens, tokens), 1)).astype(BF16)
    ahead = dot(before, count, 1, 0)
    out = []
    for k in range(top):
        rank = jnp.sum(jnp.where(hot[k], ahead, 0.0), axis=1, keepdims=True)
        out.append((cols[:, k : k + 1] * slots + rank, cols[:, top + k : top + k + 1]))
    return out


def hits(meta, experts, slots, half, rows):
    lane = (iota((meta.shape[1], rows), 1) + half * rows).astype(F32)
    found = [lane == s for s, _ in slot_of(meta, experts, slots)]
    return functools.reduce(jnp.logical_or, found).astype(BF16)


def weighted(meta, experts, slots, half, got):
    lane = (iota((meta.shape[1], got.shape[0]), 1) + half * got.shape[0]).astype(F32)
    w = jnp.zeros(lane.shape, F32)
    for s, value in slot_of(meta, experts, slots):
        w = w + jnp.where(lane == s, value, 0.0)
    high = w.astype(BF16)
    low = (w - high.astype(F32)).astype(BF16)
    return dot(high, got, 1, 0) + dot(low, got, 1, 0)


def warm_kernel(*refs):
    count = len(refs) // 2
    sem = refs[-1]
    copies = [
        pltpu.make_async_copy(refs[i], refs[count + i], sem.at[i]) for i in range(count)
    ]
    for copy in copies:
        copy.start()
    for copy in copies:
        copy.wait()


def mix_kernel(
    blocks, experts, slots, order_ref, gain_ref, fgain_ref, meta_ref, factor_ref, gate_ref,
    y_ref, cm_ref, res_ref, state_ref, *refs,
):
    count = len(blocks)
    w_refs, (mixed_ref, x_ref, send_ref) = refs[:-13], refs[-13:-10]
    wbuf, acc, vbuf, mbuf, xbuf, sbuf, sem_w, sem_m, sem_x, sem_s = refs[-10:]
    per = gate_ref.shape[1] // count
    odd = order_ref[count + 1]
    weights = []
    for i in range(count):
        weights.append([])
        for k, (which, row, size, side) in enumerate(blocks[i]):
            to = i * per
            if side is not None:
                to = to + (odd if side == 0 else 1 - odd) * size
                to = pl.multiple_of(to, size)
            copy = pltpu.make_async_copy(
                w_refs[which].at[pl.ds(row, size), :], wbuf.at[pl.ds(to, size), :], sem_w.at[i, k]
            )
            copy.start()
            weights[-1].append(copy)
    vbuf[...] = spread(factor_ref[...], gate_ref.shape[1])
    normed = []
    for i in range(count):
        wide = pl.ds(pl.multiple_of(order_ref[i] * per, per), per)
        col = pl.ds(pl.multiple_of(order_ref[i] * STATE, STATE), STATE)
        v = y_ref[:, wide] + vbuf[:, wide] * dot(cm_ref[:, col], state_ref[wide, :], 1, 1)
        v = v.astype(BF16).astype(F32)
        v = v * silu(gate_ref[:, wide].astype(F32))
        v = v * lax.rsqrt(jnp.mean(v * v, axis=1, keepdims=True) + EPS)
        normed.append((v * gain_ref[:, wide]).astype(BF16))
    features = mbuf.shape[1]
    step = features // 4
    squares = 0.0
    for i in range(0, count, 2):
        for copy in weights[i] + weights[i + 1]:
            copy.wait()
        v = jnp.concatenate(normed[i : i + 2], axis=1)
        for n in range(0, features, step):
            at = slice(n, n + step)
            out = res_ref[:, at].astype(F32) if i == 0 else acc[:, at]
            out = out + dot(v, wbuf[i * per : (i + 2) * per, at], 1, 0)
            if i < count - 2:
                acc[:, at] = out
                continue
            out = out.astype(BF16)
            mbuf[:, at] = out
            m = out.astype(F32)
            squares = squares + jnp.sum(m * m, axis=1, keepdims=True)
    out_mixed = pltpu.make_async_copy(mbuf, mixed_ref, sem_m)
    out_mixed.start()
    scale = lax.rsqrt(squares / features + EPS)
    x = (mbuf[...].astype(F32) * scale * fgain_ref[...]).astype(BF16)
    xbuf[...] = x
    out_x = pltpu.make_async_copy(xbuf, x_ref, sem_x)
    out_x.start()
    place_rows(
        hits(meta_ref[...], experts, slots, order_ref[count], send_ref.shape[0]),
        x, sbuf, send_ref, sem_s,
    )
    out_x.wait()
    out_mixed.wait()


def place_rows(hit, x, sbuf, send_ref, sem):
    pieces = sem.shape[0]
    rows = send_ref.shape[0] // pieces
    copies = []
    for i in range(pieces):
        part = slice(i * rows, (i + 1) * rows)
        sbuf[part] = dot(hit[:, part], x, 0, 0).astype(BF16)
        copies.append(
            pltpu.make_async_copy(
                sbuf.at[pl.ds(i * rows, rows)], send_ref.at[pl.ds(i * rows, rows)], sem.at[i]
            )
        )
        copies[-1].start()
    for copy in copies:
        copy.wait()


def relay_kernel(experts, slots, half_ref, meta_ref, x_in, send_ref, x_ref, sbuf, sem_x, sem):
    copy = pltpu.make_async_copy(x_in, x_ref, sem_x)
    copy.start()
    hit = hits(meta_ref[...], experts, slots, half_ref[0], send_ref.shape[0])
    copy.wait()
    place_rows(hit, x_ref[...], sbuf, send_ref, sem)


def shared_kernel(x_in, mixed_in, wg_in, wu_in, wd_in, out_ref, x_ref, m_ref, wg, wu, wd, sem):
    copies = [
        pltpu.make_async_copy(src, dst, sem.at[i])
        for i, (src, dst) in enumerate(
            ((x_in, x_ref), (wg_in, wg), (wu_in, wu), (wd_in, wd), (mixed_in, m_ref))
        )
    ]
    for copy in copies:
        copy.start()
    for copy in copies[:3]:
        copy.wait()
    x = x_ref[...]
    h = (silu(dot(x, wg[...], 1, 0)) * dot(x, wu[...], 1, 0)).astype(BF16)
    for copy in copies[3:]:
        copy.wait()
    out_ref[...] = m_ref[...].astype(F32) + dot(h, wd[...], 1, 0)


def expert_kernel(x_ref, wg_ref, wu_ref, wd_ref, out_ref, acc, obuf, sem):
    e = pl.program_id(0)
    j = pl.program_id(1)
    x = x_ref[...]
    h = (silu(dot(x, wg_ref[0], 1, 0)) * dot(x, wu_ref[0], 1, 0)).astype(BF16)
    part = dot(h, wd_ref[0], 1, 0)

    @pl.when(j == 0)
    def _():
        acc[...] = part

    @pl.when(j == pl.num_programs(1) - 1)
    def _():
        pieces = sem.shape[0]
        rows = obuf.shape[0] // pieces
        copies = []
        for i in range(pieces):
            at = slice(i * rows, (i + 1) * rows)
            obuf[at] = (acc[at] + part[at]).astype(BF16)
            copies.append(
                pltpu.make_async_copy(
                    obuf.at[pl.ds(i * rows, rows)], out_ref.at[e, pl.ds(i * rows, rows)], sem.at[i]
                )
            )
            copies[-1].start()
        for copy in copies:
            copy.wait()


def part_kernel(experts, slots, half_ref, meta_ref, got_ref, out_ref, obuf, sem):
    obuf[...] = weighted(meta_ref[...], experts, slots, half_ref[0], got_ref[...]).astype(BF16)
    copy = pltpu.make_async_copy(obuf, out_ref, sem)
    copy.start()
    copy.wait()


def combine_kernel(experts, slots, half_ref, meta_ref, got_ref, base_ref, other_ref, out_ref):
    own = weighted(meta_ref[...], experts, slots, half_ref[0], got_ref[...])
    out_ref[...] = (base_ref[...] + own + other_ref[...].astype(F32)).astype(BF16)


def gather_rows(w, ways, span):
    if ways == 4 and w.shape[0] == 2 * span and lax.axis_size("sub") % 2 == 0:
        me = lax.axis_index("dp")
        odd = lax.rem(lax.axis_index("sub"), 2).astype(jnp.int32)
        part = span // 2
        over = [(j, j ^ 2) for j in range(4)]
        core = [(j, j ^ 1) for j in range(4)]
        flip = [(j, j ^ 1) for j in range(lax.axis_size("sub"))]
        xa = lax.ppermute(lax.dynamic_slice_in_dim(w, odd * part, part, 0), "dp", over)
        xb = lax.ppermute(w[span:], "dp", over)
        ya = lax.ppermute(xa, "sub", flip)
        beside = lax.ppermute(w, "dp", core)
        fa = lax.ppermute(xa, "dp", core)
        fy = lax.ppermute(ya, "dp", core)
        fb = lax.ppermute(xb, "dp", core)
        arrays = [w, beside, xa, ya, xb, fa, fy, fb]
        blocks = [[(i, k * span, span, None)] for i in range(2) for k in range(2)]
        for i in (2, 5):
            blocks.append([(i, 0, part, 0), (i + 1, 0, part, 1)])
            blocks.append([(i + 2, 0, span, None)])
        order = [(me ^ i) * 2 + k for i in range(4) for k in range(2)]
        return arrays, blocks, order, odd
    whole = lax.all_gather(w, "dp", axis=0, tiled=True)
    count = whole.shape[0] // span
    blocks = [[(0, g * span, span, None)] for g in range(count)]
    return [whole], blocks, list(range(count)), jnp.int32(0)


def layer(
    residual, head_input, gate_input, b_input, c_input, step_input, conv_weight, conv_b_weight,
    conv_c_weight, step_bias, decay_log, skip, norm_gain, out_weight, ffn_gain, shared_gate,
    shared_up, shared_down, expert_gate, expert_up, expert_down, routes, route_weights,
):
    _, tokens, inner = head_input.shape
    features = residual.shape[2]
    heads = step_input.shape[2]
    groups = b_input.shape[2] // STATE
    top = routes.shape[2]
    ways = lax.axis_size(SP)
    ways_dp = lax.axis_size("dp")
    experts = ways * ways_dp * expert_gate.shape[0]
    slots = 2 * tokens * top // experts
    local = heads // ways
    width = local * HEAD_DIM
    span = inner // groups

    ws, blocks, order, odd = gather_rows(out_weight, ways_dp, span)
    half = lax.axis_index("half").astype(jnp.int32)
    order = jnp.stack([jnp.asarray(o, jnp.int32) for o in order + [half, odd]])
    meta = jnp.concatenate([routes[0].T.astype(F32), route_weights[0].T], axis=0)
    meta = jnp.concatenate([meta, jnp.zeros((8 - 2 * top, tokens), F32)], axis=0)
    mirror = [(0, 1), (1, 0)]
    meta_far = lax.ppermute(meta, "half", mirror)
    rows = experts * slots // 2
    pieces = 4

    hbm = pl.BlockSpec(memory_space=pltpu.HBM)
    vm = pl.BlockSpec(memory_space=pltpu.VMEM)
    x_in, b_in, c_in = head_input[0], b_input[0], c_input[0]
    turned = (step_input[0].T, step_bias[None], decay_log[None])
    tail = pl.pallas_call(
        tail_kernel,
        out_shape=jax.ShapeDtypeStruct((8, inner + 2 * b_in.shape[1]), BF16),
        in_specs=[hbm] * 3,
        out_specs=vm,
        scratch_shapes=[pltpu.SemaphoreType.DMA((3,))],
        compiler_params=vmem(60),
        cost_estimate=cost(1 << 10, 1 << 17),
        name="tails",
    )(x_in, b_in, c_in)
    tail = lax.ppermute(tail, SP, [(i, i + 1) for i in range(ways - 1)])
    fresh = pl.pallas_call(
        state_kernel,
        out_shape=pltpu.HBM((ways, width + EXTRA, STATE), BF16),
        in_specs=[vm] * 8,
        out_specs=vm,
        scratch_shapes=[
            pltpu.VMEM((8 + tokens, inner), F32),
            pltpu.VMEM((8 + tokens, b_in.shape[1]), F32),
        ],
        compiler_params=vmem(24),
        cost_estimate=cost(1 << 30, 4 * MIB),
        name="states",
    )(*turned, tail, conv_weight, conv_b_weight, x_in, b_in)
    fresh = lax.all_to_all(fresh, SP, split_axis=0, concat_axis=0, tiled=True)
    y, grow, cm = pl.pallas_call(
        inner_kernel,
        out_shape=(
            pltpu.HBM((tokens, inner), F32),
            pltpu.HBM((heads, tokens), F32),
            pltpu.HBM((tokens, b_in.shape[1]), BF16),
        ),
        in_specs=[vm] * 11,
        out_specs=(vm,) * 3,
        scratch_shapes=[
            pltpu.VMEM((8 + tokens, inner), F32),
            pltpu.VMEM((8 + tokens, b_in.shape[1]), F32),
        ],
        compiler_params=vmem(24),
        cost_estimate=cost(2 << 30, 8 * MIB),
        name="within",
    )(
        *turned, skip[None], tail, conv_weight, conv_b_weight, conv_c_weight, x_in, b_in, c_in
    )
    entering = pl.pallas_call(
        prefix_kernel,
        out_shape=jax.ShapeDtypeStruct((ways, width, STATE), BF16),
        in_specs=[vm],
        out_specs=hbm,
        scratch_shapes=[pltpu.VMEM((ways, width, STATE), BF16), pltpu.SemaphoreType.DMA((ways,))],
        compiler_params=vmem(24),
        cost_estimate=cost(1 << 26, 2 * MIB),
        name="prefix",
    )(inside(fresh))
    entering = lax.all_to_all(entering, SP, split_axis=0, concat_axis=0, tiled=True)
    entering = entering.reshape(inner, STATE)

    sm = pl.BlockSpec(memory_space=pltpu.SMEM)
    warm = [gate_input[0], y, cm, residual[0]]
    warm = pl.pallas_call(
        warm_kernel,
        out_shape=tuple(pltpu.VMEM(v.shape, v.dtype) for v in warm),
        in_specs=[hbm] * len(warm),
        out_specs=(vm,) * len(warm),
        scratch_shapes=[pltpu.SemaphoreType.DMA((len(warm),))],
        compiler_params=vmem(24),
        cost_estimate=cost(1 << 28, 8 * MIB),
        name="warm",
    )(*[outside(v) for v in warm])
    warm = [inside(v) for v in warm]
    mixed, x, send = pl.pallas_call(
        functools.partial(mix_kernel, blocks, experts, slots),
        out_shape=(
            pltpu.HBM((tokens, features), BF16),
            pltpu.HBM((tokens, features), BF16),
            pltpu.HBM((rows, features), BF16),
        ),
        in_specs=[sm] + [vm] * 9 + [hbm] * len(ws),
        out_specs=(hbm, hbm, hbm),
        scratch_shapes=[
            pltpu.VMEM((groups * span, features), BF16),
            pltpu.VMEM((tokens, features), F32),
            pltpu.VMEM((tokens, inner), F32),
            pltpu.VMEM((tokens, features), BF16),
            pltpu.VMEM((tokens, features), BF16),
            pltpu.VMEM((rows, features), BF16),
            pltpu.SemaphoreType.DMA((groups, 2)),
            pltpu.SemaphoreType.DMA,
            pltpu.SemaphoreType.DMA,
            pltpu.SemaphoreType.DMA((pieces,)),
        ],
        compiler_params=vmem(36),
        cost_estimate=cost(3 << 30, 16 * MIB),
        name="mix",
    )(
        order, norm_gain[None], ffn_gain[None], meta, grow,
        *warm, inside(entering), *[outside(v) for v in ws],
    )

    x_far = lax.ppermute(x, "half", mirror)
    group = ("sub", "dp")

    def exchange(v):
        v = v.reshape(-1, slots, features)
        return lax.all_to_all(v, group, split_axis=0, concat_axis=0, tiled=True)

    own = expert_gate.shape[0]
    ff = expert_gate.shape[2]
    bn = ff // 2

    def serve(arrived):
        if own > 1:
            arrived = arrived.reshape(-1, own, slots, features).swapaxes(0, 1)
        arrived = arrived.reshape(own, -1, features)
        m = arrived.shape[1]
        done = pl.pallas_call(
            expert_kernel,
            out_shape=jax.ShapeDtypeStruct((own, m, features), BF16),
            grid=(own, ff // bn),
            in_specs=[
                pl.BlockSpec((None, m, features), lambda e, j: (e, 0, 0)),
                pl.BlockSpec((1, features, bn), lambda e, j: (e, 0, j)),
                pl.BlockSpec((1, features, bn), lambda e, j: (e, 0, j)),
                pl.BlockSpec((1, bn, features), lambda e, j: (e, j, 0)),
            ],
            out_specs=hbm,
            scratch_shapes=[
                pltpu.VMEM((m, features), F32),
                pltpu.VMEM((m, features), BF16),
                pltpu.SemaphoreType.DMA((pieces,)),
            ],
            compiler_params=vmem(48),
            cost_estimate=cost(2 << 30, 8 * MIB),
            name="experts",
        )(arrived, expert_gate, expert_up, expert_down)
        if own > 1:
            done = done.reshape(own, -1, slots, features).swapaxes(0, 1)
        return done

    near = exchange(send)
    base = pl.pallas_call(
        shared_kernel,
        out_shape=jax.ShapeDtypeStruct((tokens, features), F32),
        in_specs=[hbm] * 5,
        out_specs=vm,
        scratch_shapes=[
            pltpu.VMEM(v.shape, BF16) for v in (x, mixed, shared_gate, shared_up, shared_down)
        ]
        + [pltpu.SemaphoreType.DMA((5,))],
        compiler_params=vmem(62),
        cost_estimate=cost(1 << 30, 8 * MIB),
        name="shared",
    )(x, mixed, shared_gate, shared_up, shared_down)
    near = serve(near)
    relay = pl.pallas_call(
        functools.partial(relay_kernel, experts, slots),
        out_shape=jax.ShapeDtypeStruct((rows, features), BF16),
        in_specs=[sm, vm, hbm],
        out_specs=hbm,
        scratch_shapes=[
            pltpu.VMEM((tokens, features), BF16),
            pltpu.VMEM((rows, features), BF16),
            pltpu.SemaphoreType.DMA,
            pltpu.SemaphoreType.DMA((pieces,)),
        ],
        compiler_params=vmem(32),
        cost_estimate=cost(1 << 28, 3 * MIB),
        name="relay",
    )(half[None], meta_far, x_far)
    far = exchange(relay)
    far = serve(far)
    far = exchange(far)
    part = pl.pallas_call(
        functools.partial(part_kernel, experts, slots),
        out_shape=jax.ShapeDtypeStruct((tokens, features), BF16),
        in_specs=[sm, vm, vm],
        out_specs=hbm,
        scratch_shapes=[pltpu.VMEM((tokens, features), BF16), pltpu.SemaphoreType.DMA],
        compiler_params=vmem(32),
        cost_estimate=cost(1 << 29, 3 * MIB),
        name="part",
    )(half[None], meta_far, far.reshape(rows, features))
    other = lax.ppermute(part, "half", mirror)
    near = exchange(near)
    out = pl.pallas_call(
        functools.partial(combine_kernel, experts, slots),
        out_shape=jax.ShapeDtypeStruct((tokens, features), BF16),
        in_specs=[sm] + [vm] * 4,
        out_specs=vm,
        compiler_params=vmem(32),
        cost_estimate=cost(1 << 29, 4 * MIB),
        name="combine",
    )(half[None], meta, near.reshape(rows, features), base, other)
    return out[None]


def solution(mesh):
    ways, ways_dp = mesh.devices.shape
    mesh = jax.sharding.Mesh(mesh.devices.reshape(2, ways // 2, ways_dp), SP + ("dp",))
    tok = P("dp", SP, None)
    exp = P(SP + ("dp",), None, None)
    return jax.shard_map(
        layer,
        mesh=mesh,
        in_specs=(tok,) * 6
        + (P(),) * 7
        + (P("dp", None),)
        + (P(),) * 4
        + (exp,) * 3
        + (tok, tok),
        out_specs=tok,
        check_vma=False,
    )
```

```python
import functools

import jax
import jax.numpy as jnp
from jax import lax
from jax.experimental import pallas as pl
from jax.experimental.pallas import tpu as pltpu
from jax.sharding import PartitionSpec as P


HEAD_DIM = 64
STATE = 128
EPS = 1e-06
HIGH = lax.Precision.HIGHEST
F32 = jnp.float32
BF16 = jnp.bfloat16
EXTRA = 8
TOP = 2
SP = ("half", "sub")
MIB = 1 << 20


def dot(a, b, ca, cb, precision=None):
    return lax.dot_general(
        a, b, (((ca,), (cb,)), ((), ())), preferred_element_type=F32, precision=precision
    )


def iota(shape, axis):
    return lax.broadcasted_iota(jnp.int32, shape, axis)


def silu(v):
    return v / (1.0 + jnp.exp(-v))


def vmem(limit):
    return pltpu.CompilerParams(vmem_limit_bytes=limit * MIB)


def inside(v):
    return pltpu.with_memory_space_constraint(v, pltpu.VMEM)


def outside(v):
    return pltpu.with_memory_space_constraint(v, pltpu.HBM)


def cost(flops, nbytes):
    return pl.CostEstimate(flops=flops, bytes_accessed=nbytes, transcendentals=0)


def tail_kernel(x_ref, b_ref, c_ref, out_ref, sem):
    copies = []
    start = 0
    rows = out_ref.shape[0]
    for i, ref in enumerate((x_ref, b_ref, c_ref)):
        size = ref.shape[1]
        copies.append(
            pltpu.make_async_copy(
                ref.at[pl.ds(ref.shape[0] - rows, rows), :],
                out_ref.at[:, pl.ds(start, size)],
                sem.at[i],
            )
        )
        copies[-1].start()
        start += size
    for copy in copies:
        copy.wait()


def conv_silu(rows_in, tail, taps, rows_ref):
    tokens = rows_in.shape[0]
    rows_ref[0:8] = tail.astype(F32)
    rows_ref[8 : 8 + tokens] = rows_in.astype(F32)
    taps = taps.astype(F32)
    act = rows_ref[8 : 8 + tokens] * taps[3:4]
    for k in range(3):
        act = act + rows_ref[5 + k : 5 + k + tokens] * taps[k : k + 1]
    return silu(act)


def decays(s_ref, bias_ref, dlog_ref):
    heads, tokens = s_ref.shape
    same = iota((heads, heads), 0) == iota((heads, heads), 1)
    bias, dlog = (
        jnp.sum(jnp.where(same, ref[...], 0.0), axis=1, keepdims=True)
        for ref in (bias_ref, dlog_ref)
    )
    pre = s_ref[...].astype(F32) + bias
    step = jnp.maximum(pre, 0.0) + jnp.log1p(jnp.exp(-jnp.abs(pre)))
    upper = (iota((tokens, tokens), 0) <= iota((tokens, tokens), 1)).astype(F32)
    cum = dot(step * -jnp.exp(dlog), upper, 1, 0, HIGH)
    return step, cum, cum[:, tokens - 1 : tokens]


def spread(v, inner):
    heads = v.shape[0]
    a = v.astype(BF16)
    rest = v - a.astype(F32)
    b = rest.astype(BF16)
    c = (rest - b.astype(F32)).astype(BF16)
    own = (iota((heads, inner), 0) == iota((heads, inner), 1) // HEAD_DIM).astype(BF16)
    return dot(jnp.concatenate([a, b, c], axis=0), jnp.concatenate([own] * 3, axis=0), 0, 0)


def state_kernel(
    s_ref, bias_ref, dlog_ref, tail_ref, wx_ref, wb_ref, x_ref, b_ref, out_ref, rx_ref, rb_ref
):
    inner = x_ref.shape[1]
    ways = out_ref.shape[0]
    rows = out_ref.shape[1] - EXTRA
    local = rows // HEAD_DIM
    span = inner // (b_ref.shape[1] // STATE)
    step, cum, total = decays(s_ref, bias_ref, dlog_ref)
    wide = spread(step * jnp.exp(total - cum), inner)
    fade = jnp.exp(jnp.broadcast_to(total, (total.shape[0], STATE)))
    high = fade.astype(BF16).astype(F32)
    low = fade - high
    bm = conv_silu(b_ref[...], tail_ref[:, inner : inner + b_ref.shape[1]], wb_ref[...], rb_ref)
    bm = bm.astype(BF16)
    xs = conv_silu(x_ref[...], tail_ref[:, :inner], wx_ref[...], rx_ref)
    xw = (xs * wide).astype(BF16)
    blank = jnp.zeros((EXTRA // 2 - local, STATE), F32)
    for d in range(ways):
        g = d * rows // span
        st = dot(xw[:, d * rows : (d + 1) * rows], bm[:, g * STATE : (g + 1) * STATE], 0, 0)
        out_ref[d, 0:rows, :] = st.astype(BF16)
        own = slice(d * local, (d + 1) * local)
        parts = [high[own], low[own]]
        if local < EXTRA // 2:
            parts = [high[own], blank, low[own], blank]
        out_ref[d, rows : rows + EXTRA, :] = jnp.concatenate(parts, axis=0).astype(BF16)


def prefix_kernel(in_ref, out_hbm, out_ref, sem_out):
    ways, rows, _ = out_ref.shape
    puts = [pltpu.make_async_copy(out_ref.at[j], out_hbm.at[j], sem_out.at[j]) for j in range(ways)]
    state = jnp.zeros((rows, STATE), F32)
    for j in range(ways):
        fade = in_ref[j, rows : rows + EXTRA, :].astype(F32)
        old = jnp.concatenate(
            [
                state[h * HEAD_DIM : (h + 1) * HEAD_DIM]
                * (fade[h : h + 1] + fade[h + EXTRA // 2 : h + 1 + EXTRA // 2])
                for h in range(rows // HEAD_DIM)
            ],
            axis=0,
        )
        out_ref[j] = old.astype(BF16)
        puts[j].start()
        state = old + in_ref[j, 0:rows, :].astype(F32)
    for put in puts:
        put.wait()


def inner_kernel(
    s_ref, bias_ref, dlog_ref, skip_ref, tail_ref, wx_ref, wb_ref, wc_ref, x_ref, b_ref, c_ref,
    y_ref, grow_ref, cm_ref, rx_ref, rb_ref,
):
    tokens, inner = x_ref.shape
    heads = s_ref.shape[0]
    narrow = b_ref.shape[1]
    groups = narrow // STATE
    span = inner // groups
    step, cum, total = decays(s_ref, bias_ref, dlog_ref)
    wide = spread(step * jnp.exp(total - cum), inner)
    grow_ref[...] = jnp.exp(cum - total)
    grow = spread(grow_ref[...], inner)
    own = (iota((heads, inner), 0) == iota((heads, inner), 1) // HEAD_DIM).astype(F32)
    skip = dot(skip_ref[...], own, 1, 0, HIGH)
    bm = conv_silu(b_ref[...], tail_ref[:, inner : inner + narrow], wb_ref[...], rb_ref)
    bm = bm.astype(BF16)
    cm = conv_silu(c_ref[...], tail_ref[:, inner + narrow :], wc_ref[...], rb_ref).astype(BF16)
    cm_ref[...] = cm
    xs = conv_silu(x_ref[...], tail_ref[:, :inner], wx_ref[...], rx_ref)
    xw = (xs * wide).astype(BF16)
    lower = iota((tokens, tokens), 0) >= iota((tokens, tokens), 1)
    for g in range(groups):
        n = slice(g * STATE, (g + 1) * STATE)
        at = slice(g * span, (g + 1) * span)
        scores = jnp.where(lower, dot(cm[:, n], bm[:, n], 1, 1), 0.0).astype(BF16)
        y_ref[:, at] = grow[:, at] * dot(scores, xw[:, at], 1, 0) + skip[:, at] * xs[:, at]


def slot_of(meta, experts, slots):
    tokens = meta.shape[1]
    top = TOP
    same = (iota((tokens, tokens), 0) == iota((tokens, tokens), 1)).astype(F32)
    cols = dot(same, meta, 1, 1, HIGH)
    lane = iota((tokens, experts), 1).astype(F32)
    hot = [lane == cols[:, k : k + 1] for k in range(top)]
    count = sum(h.astype(F32) for h in hot).astype(BF16)
    before = (iota((tokens, tokens), 0) > iota((tokens, tokens), 1)).astype(BF16)
    ahead = dot(before, count, 1, 0)
    out = []
    for k in range(top):
        rank = jnp.sum(jnp.where(hot[k], ahead, 0.0), axis=1, keepdims=True)
        out.append((cols[:, k : k + 1] * slots + rank, cols[:, top + k : top + k + 1]))
    return out


def hits(meta, experts, slots, half, rows):
    lane = (iota((meta.shape[1], rows), 1) + half * rows).astype(F32)
    found = [lane == s for s, _ in slot_of(meta, experts, slots)]
    return functools.reduce(jnp.logical_or, found).astype(BF16)


def shares(meta, experts, slots, half, rows):
    lane = (iota((meta.shape[1], rows), 1) + half * rows).astype(F32)
    w = jnp.zeros(lane.shape, F32)
    for s, value in slot_of(meta, experts, slots):
        w = w + jnp.where(lane == s, value, 0.0)
    high = w.astype(BF16)
    return high, (w - high.astype(F32)).astype(BF16)


def weighted(shares_ref, got):
    return dot(shares_ref[0], got, 1, 0) + dot(shares_ref[1], got, 1, 0)


def plan_kernel(experts, slots, half_ref, meta_ref, far_ref, hit_ref, near_ref, over_ref):
    rows = hit_ref.shape[1]
    half = half_ref[0]
    hit_ref[...] = hits(far_ref[...], experts, slots, half, rows)
    for meta, ref in ((meta_ref, near_ref), (far_ref, over_ref)):
        ref[0], ref[1] = shares(meta[...], experts, slots, half, rows)


def warm_kernel(*refs):
    count = len(refs) // 2
    sem = refs[-1]
    copies = [
        pltpu.make_async_copy(refs[i], refs[count + i], sem.at[i]) for i in range(count)
    ]
    for copy in copies:
        copy.start()
    for copy in copies:
        copy.wait()


def mix_kernel(
    blocks, experts, slots, order_ref, gain_ref, fgain_ref, meta_ref, factor_ref, gate_ref,
    y_ref, cm_ref, res_ref, state_ref, *refs,
):
    count = len(blocks)
    w_refs, (mixed_ref, x_ref, send_ref) = refs[:-13], refs[-13:-10]
    wbuf, acc, vbuf, mbuf, xbuf, sbuf, sem_w, sem_m, sem_x, sem_s = refs[-10:]
    per = gate_ref.shape[1] // count
    odd = order_ref[count + 1]
    weights = []
    for i in range(count):
        weights.append([])
        for k, (which, row, size, side) in enumerate(blocks[i]):
            to = i * per
            if side is not None:
                to = to + (odd if side == 0 else 1 - odd) * size
                to = pl.multiple_of(to, size)
            copy = pltpu.make_async_copy(
                w_refs[which].at[pl.ds(row, size), :], wbuf.at[pl.ds(to, size), :], sem_w.at[i, k]
            )
            copy.start()
            weights[-1].append(copy)
    vbuf[...] = spread(factor_ref[...], gate_ref.shape[1])
    normed = []
    for i in range(count):
        wide = pl.ds(pl.multiple_of(order_ref[i] * per, per), per)
        col = pl.ds(pl.multiple_of(order_ref[i] * STATE, STATE), STATE)
        v = y_ref[:, wide] + vbuf[:, wide] * dot(cm_ref[:, col], state_ref[wide, :], 1, 1)
        v = v.astype(BF16).astype(F32)
        v = v * silu(gate_ref[:, wide].astype(F32))
        v = v * lax.rsqrt(jnp.mean(v * v, axis=1, keepdims=True) + EPS)
        normed.append((v * gain_ref[:, wide]).astype(BF16))
    features = mbuf.shape[1]
    step = features // 4
    squares = 0.0
    for i in range(0, count, 2):
        for copy in weights[i] + weights[i + 1]:
            copy.wait()
        v = jnp.concatenate(normed[i : i + 2], axis=1)
        for n in range(0, features, step):
            at = slice(n, n + step)
            out = res_ref[:, at].astype(F32) if i == 0 else acc[:, at]
            out = out + dot(v, wbuf[i * per : (i + 2) * per, at], 1, 0)
            if i < count - 2:
                acc[:, at] = out
                continue
            out = out.astype(BF16)
            mbuf[:, at] = out
            m = out.astype(F32)
            squares = squares + jnp.sum(m * m, axis=1, keepdims=True)
    out_mixed = pltpu.make_async_copy(mbuf, mixed_ref, sem_m)
    out_mixed.start()
    scale = lax.rsqrt(squares / features + EPS)
    x = (mbuf[...].astype(F32) * scale * fgain_ref[...]).astype(BF16)
    xbuf[...] = x
    out_x = pltpu.make_async_copy(xbuf, x_ref, sem_x)
    out_x.start()
    place_rows(
        hits(meta_ref[...], experts, slots, order_ref[count], send_ref.shape[0]),
        x, sbuf, send_ref, sem_s,
    )
    out_x.wait()
    out_mixed.wait()


def place_rows(hit, x, sbuf, send_ref, sem):
    pieces = sem.shape[0]
    rows = send_ref.shape[0] // pieces
    copies = []
    for i in range(pieces):
        part = slice(i * rows, (i + 1) * rows)
        sbuf[part] = dot(hit[:, part], x, 0, 0).astype(BF16)
        copies.append(
            pltpu.make_async_copy(
                sbuf.at[pl.ds(i * rows, rows)], send_ref.at[pl.ds(i * rows, rows)], sem.at[i]
            )
        )
        copies[-1].start()
    for copy in copies:
        copy.wait()


def relay_kernel(hit_ref, x_in, send_ref, x_ref, sbuf, sem_x, sem):
    pieces = sem.shape[0]
    step = x_ref.shape[1] // pieces
    wide = [pl.ds(i * step, step) for i in range(pieces)]
    gets = [pltpu.make_async_copy(x_in.at[:, w], x_ref.at[:, w], sem_x.at[i]) for i, w in enumerate(wide)]
    puts = [pltpu.make_async_copy(sbuf.at[:, w], send_ref.at[:, w], sem.at[i]) for i, w in enumerate(wide)]
    for get in gets:
        get.start()
    hit = hit_ref[...]
    for i in range(pieces):
        gets[i].wait()
        at = slice(i * step, (i + 1) * step)
        sbuf[:, at] = dot(hit, x_ref[:, at], 0, 0).astype(BF16)
        puts[i].start()
    for put in puts:
        put.wait()


def shared_kernel(x_in, mixed_in, wg_in, wu_in, wd_in, out_ref, x_ref, m_ref, wg, wu, wd, sem):
    copies = [
        pltpu.make_async_copy(src, dst, sem.at[i])
        for i, (src, dst) in enumerate(
            ((x_in, x_ref), (wg_in, wg), (wu_in, wu), (wd_in, wd), (mixed_in, m_ref))
        )
    ]
    for copy in copies:
        copy.start()
    for copy in copies[:3]:
        copy.wait()
    x = x_ref[...]
    h = (silu(dot(x, wg[...], 1, 0)) * dot(x, wu[...], 1, 0)).astype(BF16)
    for copy in copies[3:]:
        copy.wait()
    out_ref[...] = m_ref[...].astype(F32) + dot(h, wd[...], 1, 0)


def expert_kernel(x_ref, wg_ref, wu_ref, wd_ref, out_ref, acc, obuf, sem):
    e = pl.program_id(0)
    j = pl.program_id(1)
    x = x_ref[...]
    h = (silu(dot(x, wg_ref[0], 1, 0)) * dot(x, wu_ref[0], 1, 0)).astype(BF16)
    part = dot(h, wd_ref[0], 1, 0)

    @pl.when(j == 0)
    def _():
        acc[...] = part

    @pl.when(j == pl.num_programs(1) - 1)
    def _():
        pieces = sem.shape[0]
        rows = obuf.shape[0] // pieces
        copies = []
        for i in range(pieces):
            at = slice(i * rows, (i + 1) * rows)
            obuf[at] = (acc[at] + part[at]).astype(BF16)
            copies.append(
                pltpu.make_async_copy(
                    obuf.at[pl.ds(i * rows, rows)], out_ref.at[e, pl.ds(i * rows, rows)], sem.at[i]
                )
            )
            copies[-1].start()
        for copy in copies:
            copy.wait()


def part_kernel(shares_ref, got_ref, out_ref, obuf, sem):
    obuf[...] = weighted(shares_ref, got_ref[...]).astype(BF16)
    copy = pltpu.make_async_copy(obuf, out_ref, sem)
    copy.start()
    copy.wait()


def sum_kernel(base_ref, other_ref, out_ref):
    out_ref[...] = base_ref[...] + other_ref[...].astype(F32)


def combine_kernel(shares_ref, got_ref, base_ref, out_ref):
    out_ref[...] = (base_ref[...] + weighted(shares_ref, got_ref[...])).astype(BF16)


def gather_rows(w, ways, span):
    if ways == 4 and w.shape[0] == 2 * span and lax.axis_size("sub") % 2 == 0:
        me = lax.axis_index("dp")
        odd = lax.rem(lax.axis_index("sub"), 2).astype(jnp.int32)
        part = span // 2
        over = [(j, j ^ 2) for j in range(4)]
        core = [(j, j ^ 1) for j in range(4)]
        flip = [(j, j ^ 1) for j in range(lax.axis_size("sub"))]
        xa = lax.ppermute(lax.dynamic_slice_in_dim(w, odd * part, part, 0), "dp", over)
        low = w[span:]
        xb = lax.ppermute(low, "dp", over)
        ya = lax.ppermute(xa, "sub", flip)
        beside = lax.ppermute(w, "dp", core)
        fa = lax.ppermute(xa, "dp", core)
        fy = lax.ppermute(ya, "dp", core)
        fb = lax.ppermute(xb, "dp", core)
        arrays = [w, beside, xa, ya, xb, fa, fy, fb]
        blocks = [[(i, k * span, span, None)] for i in range(2) for k in range(2)]
        for i in (2, 5):
            blocks.append([(i, 0, part, 0), (i + 1, 0, part, 1)])
            blocks.append([(i + 2, 0, span, None)])
        order = [(me ^ i) * 2 + k for i in range(4) for k in range(2)]
        return arrays, blocks, order, odd
    whole = lax.all_gather(w, "dp", axis=0, tiled=True)
    count = whole.shape[0] // span
    blocks = [[(0, g * span, span, None)] for g in range(count)]
    return [whole], blocks, list(range(count)), jnp.int32(0)


def layer(
    residual, head_input, gate_input, b_input, c_input, step_input, conv_weight, conv_b_weight,
    conv_c_weight, step_bias, decay_log, skip, norm_gain, out_weight, ffn_gain, shared_gate,
    shared_up, shared_down, expert_gate, expert_up, expert_down, routes, route_weights,
):
    _, tokens, inner = head_input.shape
    features = residual.shape[2]
    heads = step_input.shape[2]
    groups = b_input.shape[2] // STATE
    top = routes.shape[2]
    ways = lax.axis_size(SP)
    ways_dp = lax.axis_size("dp")
    experts = ways * ways_dp * expert_gate.shape[0]
    slots = 2 * tokens * top // experts
    local = heads // ways
    width = local * HEAD_DIM
    span = inner // groups

    ws, blocks, order, odd = gather_rows(out_weight, ways_dp, span)
    half = lax.axis_index("half").astype(jnp.int32)
    order = jnp.stack([jnp.asarray(o, jnp.int32) for o in order + [half, odd]])
    meta = jnp.concatenate([routes[0].T.astype(F32), route_weights[0].T], axis=0)
    meta = jnp.concatenate([meta, jnp.zeros((8 - 2 * top, tokens), F32)], axis=0)
    mirror = [(0, 1), (1, 0)]
    meta_far = lax.ppermute(meta, "half", mirror)
    rows = experts * slots // 2
    pieces = 4

    hbm = pl.BlockSpec(memory_space=pltpu.HBM)
    vm = pl.BlockSpec(memory_space=pltpu.VMEM)
    x_in, b_in, c_in = head_input[0], b_input[0], c_input[0]
    turned = (step_input[0].T, step_bias[None], decay_log[None])
    tail = pl.pallas_call(
        tail_kernel,
        out_shape=jax.ShapeDtypeStruct((8, inner + 2 * b_in.shape[1]), BF16),
        in_specs=[hbm] * 3,
        out_specs=vm,
        scratch_shapes=[pltpu.SemaphoreType.DMA((3,))],
        compiler_params=vmem(60),
        cost_estimate=cost(1 << 10, 1 << 17),
        name="tails",
    )(x_in, b_in, c_in)
    tail = lax.ppermute(tail, SP, [(i, i + 1) for i in range(ways - 1)])
    fresh = pl.pallas_call(
        state_kernel,
        out_shape=pltpu.HBM((ways, width + EXTRA, STATE), BF16),
        in_specs=[vm] * 8,
        out_specs=vm,
        scratch_shapes=[
            pltpu.VMEM((8 + tokens, inner), F32),
            pltpu.VMEM((8 + tokens, b_in.shape[1]), F32),
        ],
        compiler_params=vmem(24),
        cost_estimate=cost(1 << 30, 4 * MIB),
        name="states",
    )(*turned, tail, conv_weight, conv_b_weight, x_in, b_in)
    fresh = lax.all_to_all(fresh, SP, split_axis=0, concat_axis=0, tiled=True)
    y, grow, cm = pl.pallas_call(
        inner_kernel,
        out_shape=(
            pltpu.HBM((tokens, inner), F32),
            pltpu.HBM((heads, tokens), F32),
            pltpu.HBM((tokens, b_in.shape[1]), BF16),
        ),
        in_specs=[vm] * 11,
        out_specs=(vm,) * 3,
        scratch_shapes=[
            pltpu.VMEM((8 + tokens, inner), F32),
            pltpu.VMEM((8 + tokens, b_in.shape[1]), F32),
        ],
        compiler_params=vmem(24),
        cost_estimate=cost(2 << 30, 8 * MIB),
        name="within",
    )(
        *turned, skip[None], tail, conv_weight, conv_b_weight, conv_c_weight, x_in, b_in, c_in
    )
    entering = pl.pallas_call(
        prefix_kernel,
        out_shape=jax.ShapeDtypeStruct((ways, width, STATE), BF16),
        in_specs=[vm],
        out_specs=hbm,
        scratch_shapes=[pltpu.VMEM((ways, width, STATE), BF16), pltpu.SemaphoreType.DMA((ways,))],
        compiler_params=vmem(24),
        cost_estimate=cost(1 << 26, 2 * MIB),
        name="prefix",
    )(inside(fresh))
    entering = lax.all_to_all(entering, SP, split_axis=0, concat_axis=0, tiled=True)
    entering = entering.reshape(inner, STATE)

    sm = pl.BlockSpec(memory_space=pltpu.SMEM)
    warm = [gate_input[0], y, cm, residual[0]]
    warm = pl.pallas_call(
        warm_kernel,
        out_shape=tuple(pltpu.VMEM(v.shape, v.dtype) for v in warm),
        in_specs=[hbm] * len(warm),
        out_specs=(vm,) * len(warm),
        scratch_shapes=[pltpu.SemaphoreType.DMA((len(warm),))],
        compiler_params=vmem(24),
        cost_estimate=cost(1 << 28, 8 * MIB),
        name="warm",
    )(*[outside(v) for v in warm])
    warm = [inside(v) for v in warm]
    mixed, x, send = pl.pallas_call(
        functools.partial(mix_kernel, blocks, experts, slots),
        out_shape=(
            pltpu.HBM((tokens, features), BF16),
            pltpu.HBM((tokens, features), BF16),
            pltpu.HBM((rows, features), BF16),
        ),
        in_specs=[sm] + [vm] * 9 + [hbm] * len(ws),
        out_specs=(hbm, hbm, hbm),
        scratch_shapes=[
            pltpu.VMEM((groups * span, features), BF16),
            pltpu.VMEM((tokens, features), F32),
            pltpu.VMEM((tokens, inner), F32),
            pltpu.VMEM((tokens, features), BF16),
            pltpu.VMEM((tokens, features), BF16),
            pltpu.VMEM((rows, features), BF16),
            pltpu.SemaphoreType.DMA((groups, 2)),
            pltpu.SemaphoreType.DMA,
            pltpu.SemaphoreType.DMA,
            pltpu.SemaphoreType.DMA((pieces,)),
        ],
        compiler_params=vmem(36),
        cost_estimate=cost(3 << 30, 16 * MIB),
        name="mix",
    )(
        order, norm_gain[None], ffn_gain[None], meta, grow,
        *warm, inside(entering), *[outside(v) for v in ws],
    )

    x_far = lax.ppermute(x, "half", mirror)
    group = ("sub", "dp")

    def exchange(v):
        v = v.reshape(-1, slots, features)
        return lax.all_to_all(v, group, split_axis=0, concat_axis=0, tiled=True)

    own = expert_gate.shape[0]
    ff = expert_gate.shape[2]
    bn = ff // 2

    def serve(arrived):
        if own > 1:
            arrived = arrived.reshape(-1, own, slots, features).swapaxes(0, 1)
        arrived = arrived.reshape(own, -1, features)
        m = arrived.shape[1]
        done = pl.pallas_call(
            expert_kernel,
            out_shape=jax.ShapeDtypeStruct((own, m, features), BF16),
            grid=(own, ff // bn),
            in_specs=[
                pl.BlockSpec((None, m, features), lambda e, j: (e, 0, 0)),
                pl.BlockSpec((1, features, bn), lambda e, j: (e, 0, j)),
                pl.BlockSpec((1, features, bn), lambda e, j: (e, 0, j)),
                pl.BlockSpec((1, bn, features), lambda e, j: (e, j, 0)),
            ],
            out_specs=hbm,
            scratch_shapes=[
                pltpu.VMEM((m, features), F32),
                pltpu.VMEM((m, features), BF16),
                pltpu.SemaphoreType.DMA((pieces,)),
            ],
            compiler_params=vmem(48),
            cost_estimate=cost(2 << 30, 8 * MIB),
            name="experts",
        )(arrived, expert_gate, expert_up, expert_down)
        if own > 1:
            done = done.reshape(own, -1, slots, features).swapaxes(0, 1)
        return done

    near = exchange(send)
    base = pl.pallas_call(
        shared_kernel,
        out_shape=jax.ShapeDtypeStruct((tokens, features), F32),
        in_specs=[hbm] * 5,
        out_specs=vm,
        scratch_shapes=[
            pltpu.VMEM(v.shape, BF16) for v in (x, mixed, shared_gate, shared_up, shared_down)
        ]
        + [pltpu.SemaphoreType.DMA((5,))],
        compiler_params=vmem(62),
        cost_estimate=cost(1 << 30, 8 * MIB),
        name="shared",
    )(x, mixed, shared_gate, shared_up, shared_down)
    near = serve(near)
    hit_far, near_shares, far_shares = pl.pallas_call(
        functools.partial(plan_kernel, experts, slots),
        out_shape=(
            jax.ShapeDtypeStruct((tokens, rows), BF16),
            jax.ShapeDtypeStruct((2, tokens, rows), BF16),
            jax.ShapeDtypeStruct((2, tokens, rows), BF16),
        ),
        in_specs=[sm, vm, vm],
        out_specs=(vm,) * 3,
        compiler_params=vmem(24),
        cost_estimate=cost(1 << 27, 1 << 19),
        name="plan",
    )(half[None], meta, meta_far)
    relay = pl.pallas_call(
        relay_kernel,
        out_shape=pltpu.HBM((rows, features), BF16),
        in_specs=[vm, hbm],
        out_specs=hbm,
        scratch_shapes=[
            pltpu.VMEM((tokens, features), BF16),
            pltpu.VMEM((rows, features), BF16),
            pltpu.SemaphoreType.DMA((pieces,)),
            pltpu.SemaphoreType.DMA((pieces,)),
        ],
        compiler_params=vmem(32),
        cost_estimate=cost(1 << 28, 3 * MIB),
        name="relay",
    )(hit_far, x_far)
    far = exchange(relay)
    far = serve(far)
    far = exchange(far)
    part = pl.pallas_call(
        part_kernel,
        out_shape=pltpu.HBM((tokens, features), BF16),
        in_specs=[vm, vm],
        out_specs=hbm,
        scratch_shapes=[pltpu.VMEM((tokens, features), BF16), pltpu.SemaphoreType.DMA],
        compiler_params=vmem(32),
        cost_estimate=cost(1 << 29, 3 * MIB),
        name="part",
    )(far_shares, far.reshape(rows, features))
    other = lax.ppermute(part, "half", mirror)
    near = exchange(near)
    base = pl.pallas_call(
        sum_kernel,
        out_shape=jax.ShapeDtypeStruct((tokens, features), F32),
        in_specs=[vm, vm],
        out_specs=vm,
        compiler_params=vmem(32),
        cost_estimate=cost(1 << 20, 3 * MIB),
        name="sum",
    )(base, other)
    out = pl.pallas_call(
        combine_kernel,
        out_shape=jax.ShapeDtypeStruct((tokens, features), BF16),
        in_specs=[vm] * 3,
        out_specs=vm,
        compiler_params=vmem(32),
        cost_estimate=cost(1 << 29, 4 * MIB),
        name="combine",
    )(near_shares, near.reshape(rows, features), base)
    return out[None]


def solution(mesh):
    ways, ways_dp = mesh.devices.shape
    mesh = jax.sharding.Mesh(mesh.devices.reshape(2, ways // 2, ways_dp), SP + ("dp",))
    tok = P("dp", SP, None)
    exp = P(SP + ("dp",), None, None)
    return jax.shard_map(
        layer,
        mesh=mesh,
        in_specs=(tok,) * 6
        + (P(),) * 7
        + (P("dp", None),)
        + (P(),) * 4
        + (exp,) * 3
        + (tok, tok),
        out_specs=tok,
        check_vma=False,
    )
```

```python
import functools

import jax
import jax.numpy as jnp
from jax import lax
from jax.experimental import pallas as pl
from jax.experimental.pallas import tpu as pltpu
from jax.sharding import PartitionSpec as P


HEAD_DIM = 64
STATE = 128
EPS = 1e-06
HIGH = lax.Precision.HIGHEST
F32 = jnp.float32
BF16 = jnp.bfloat16
EXTRA = 8
TOP = 2
SP = ("half", "sub")
MIB = 1 << 20


def dot(a, b, ca, cb, precision=None):
    return lax.dot_general(
        a, b, (((ca,), (cb,)), ((), ())), preferred_element_type=F32, precision=precision
    )


def iota(shape, axis):
    return lax.broadcasted_iota(jnp.int32, shape, axis)


def silu(v):
    return v / (1.0 + jnp.exp(-v))


def vmem(limit):
    return pltpu.CompilerParams(vmem_limit_bytes=limit * MIB)


def inside(v):
    return pltpu.with_memory_space_constraint(v, pltpu.VMEM)


def outside(v):
    return pltpu.with_memory_space_constraint(v, pltpu.HBM)


def cost(flops, nbytes):
    return pl.CostEstimate(flops=flops, bytes_accessed=nbytes, transcendentals=0)


def tail_kernel(x_ref, b_ref, c_ref, out_ref, sem):
    copies = []
    start = 0
    rows = out_ref.shape[0]
    for i, ref in enumerate((x_ref, b_ref, c_ref)):
        size = ref.shape[1]
        copies.append(
            pltpu.make_async_copy(
                ref.at[pl.ds(ref.shape[0] - rows, rows), :],
                out_ref.at[:, pl.ds(start, size)],
                sem.at[i],
            )
        )
        copies[-1].start()
        start += size
    for copy in copies:
        copy.wait()


def conv_silu(rows_in, tail, taps, rows_ref):
    tokens = rows_in.shape[0]
    rows_ref[0:8] = tail.astype(F32)
    rows_ref[8 : 8 + tokens] = rows_in.astype(F32)
    taps = taps.astype(F32)
    act = rows_ref[8 : 8 + tokens] * taps[3:4]
    for k in range(3):
        act = act + rows_ref[5 + k : 5 + k + tokens] * taps[k : k + 1]
    return silu(act)


def decays(s_ref, bias_ref, dlog_ref):
    heads, tokens = s_ref.shape
    same = iota((heads, heads), 0) == iota((heads, heads), 1)
    bias, dlog = (
        jnp.sum(jnp.where(same, ref[...], 0.0), axis=1, keepdims=True)
        for ref in (bias_ref, dlog_ref)
    )
    pre = s_ref[...].astype(F32) + bias
    step = jnp.maximum(pre, 0.0) + jnp.log1p(jnp.exp(-jnp.abs(pre)))
    upper = (iota((tokens, tokens), 0) <= iota((tokens, tokens), 1)).astype(F32)
    cum = dot(step * -jnp.exp(dlog), upper, 1, 0, HIGH)
    return step, cum, cum[:, tokens - 1 : tokens]


def spread(v, inner):
    heads = v.shape[0]
    a = v.astype(BF16)
    rest = v - a.astype(F32)
    b = rest.astype(BF16)
    c = (rest - b.astype(F32)).astype(BF16)
    own = (iota((heads, inner), 0) == iota((heads, inner), 1) // HEAD_DIM).astype(BF16)
    return dot(jnp.concatenate([a, b, c], axis=0), jnp.concatenate([own] * 3, axis=0), 0, 0)


def state_kernel(
    s_ref, bias_ref, dlog_ref, tail_ref, wx_ref, wb_ref, x_ref, b_ref, out_ref, rx_ref, rb_ref
):
    inner = x_ref.shape[1]
    ways = out_ref.shape[0]
    rows = out_ref.shape[1] - EXTRA
    local = rows // HEAD_DIM
    span = inner // (b_ref.shape[1] // STATE)
    step, cum, total = decays(s_ref, bias_ref, dlog_ref)
    wide = spread(step * jnp.exp(total - cum), inner)
    fade = jnp.exp(jnp.broadcast_to(total, (total.shape[0], STATE)))
    high = fade.astype(BF16).astype(F32)
    low = fade - high
    bm = conv_silu(b_ref[...], tail_ref[:, inner : inner + b_ref.shape[1]], wb_ref[...], rb_ref)
    bm = bm.astype(BF16)
    xs = conv_silu(x_ref[...], tail_ref[:, :inner], wx_ref[...], rx_ref)
    xw = (xs * wide).astype(BF16)
    blank = jnp.zeros((EXTRA // 2 - local, STATE), F32)
    for d in range(ways):
        g = d * rows // span
        st = dot(xw[:, d * rows : (d + 1) * rows], bm[:, g * STATE : (g + 1) * STATE], 0, 0)
        out_ref[d, 0:rows, :] = st.astype(BF16)
        own = slice(d * local, (d + 1) * local)
        parts = [high[own], low[own]]
        if local < EXTRA // 2:
            parts = [high[own], blank, low[own], blank]
        out_ref[d, rows : rows + EXTRA, :] = jnp.concatenate(parts, axis=0).astype(BF16)


def prefix_kernel(in_ref, out_hbm, out_ref, sem_out):
    ways, rows, _ = out_ref.shape
    puts = [pltpu.make_async_copy(out_ref.at[j], out_hbm.at[j], sem_out.at[j]) for j in range(ways)]
    state = jnp.zeros((rows, STATE), F32)
    for j in range(ways):
        fade = in_ref[j, rows : rows + EXTRA, :].astype(F32)
        old = jnp.concatenate(
            [
                state[h * HEAD_DIM : (h + 1) * HEAD_DIM]
                * (fade[h : h + 1] + fade[h + EXTRA // 2 : h + 1 + EXTRA // 2])
                for h in range(rows // HEAD_DIM)
            ],
            axis=0,
        )
        out_ref[j] = old.astype(BF16)
        puts[j].start()
        state = old + in_ref[j, 0:rows, :].astype(F32)
    for put in puts:
        put.wait()


def inner_kernel(
    s_ref, bias_ref, dlog_ref, skip_ref, tail_ref, wx_ref, wb_ref, wc_ref, x_ref, b_ref, c_ref,
    y_ref, grow_ref, cm_ref, rx_ref, rb_ref,
):
    tokens, inner = x_ref.shape
    heads = s_ref.shape[0]
    narrow = b_ref.shape[1]
    groups = narrow // STATE
    span = inner // groups
    step, cum, total = decays(s_ref, bias_ref, dlog_ref)
    wide = spread(step * jnp.exp(total - cum), inner)
    grow_ref[...] = jnp.exp(cum - total)
    grow = spread(grow_ref[...], inner)
    own = (iota((heads, inner), 0) == iota((heads, inner), 1) // HEAD_DIM).astype(F32)
    skip = dot(skip_ref[...], own, 1, 0, HIGH)
    bm = conv_silu(b_ref[...], tail_ref[:, inner : inner + narrow], wb_ref[...], rb_ref)
    bm = bm.astype(BF16)
    cm = conv_silu(c_ref[...], tail_ref[:, inner + narrow :], wc_ref[...], rb_ref).astype(BF16)
    cm_ref[...] = cm
    xs = conv_silu(x_ref[...], tail_ref[:, :inner], wx_ref[...], rx_ref)
    xw = (xs * wide).astype(BF16)
    lower = iota((tokens, tokens), 0) >= iota((tokens, tokens), 1)
    for g in range(groups):
        n = slice(g * STATE, (g + 1) * STATE)
        at = slice(g * span, (g + 1) * span)
        scores = jnp.where(lower, dot(cm[:, n], bm[:, n], 1, 1), 0.0).astype(BF16)
        y_ref[:, at] = grow[:, at] * dot(scores, xw[:, at], 1, 0) + skip[:, at] * xs[:, at]


def slot_of(meta, experts, slots):
    tokens = meta.shape[1]
    top = TOP
    same = (iota((tokens, tokens), 0) == iota((tokens, tokens), 1)).astype(F32)
    cols = dot(same, meta, 1, 1, HIGH)
    lane = iota((tokens, experts), 1).astype(F32)
    hot = [lane == cols[:, k : k + 1] for k in range(top)]
    count = sum(h.astype(F32) for h in hot).astype(BF16)
    before = (iota((tokens, tokens), 0) > iota((tokens, tokens), 1)).astype(BF16)
    ahead = dot(before, count, 1, 0)
    out = []
    for k in range(top):
        rank = jnp.sum(jnp.where(hot[k], ahead, 0.0), axis=1, keepdims=True)
        out.append((cols[:, k : k + 1] * slots + rank, cols[:, top + k : top + k + 1]))
    return out


def hits(meta, experts, slots, half, rows):
    lane = (iota((meta.shape[1], rows), 1) + half * rows).astype(F32)
    found = [lane == s for s, _ in slot_of(meta, experts, slots)]
    return functools.reduce(jnp.logical_or, found).astype(BF16)


def shares(meta, experts, slots, half, rows):
    lane = (iota((meta.shape[1], rows), 1) + half * rows).astype(F32)
    w = jnp.zeros(lane.shape, F32)
    for s, value in slot_of(meta, experts, slots):
        w = w + jnp.where(lane == s, value, 0.0)
    high = w.astype(BF16)
    return high, (w - high.astype(F32)).astype(BF16)


def weighted(shares_ref, got):
    return dot(shares_ref[0], got, 1, 0) + dot(shares_ref[1], got, 1, 0)


def plan_kernel(experts, slots, half_ref, meta_ref, far_ref, hit_ref, near_ref, over_ref):
    rows = hit_ref.shape[1]
    half = half_ref[0]
    hit_ref[...] = hits(far_ref[...], experts, slots, half, rows)
    for meta, ref in ((meta_ref, near_ref), (far_ref, over_ref)):
        ref[0], ref[1] = shares(meta[...], experts, slots, half, rows)


def warm_kernel(*refs):
    count = len(refs) // 2
    sem = refs[-1]
    copies = [
        pltpu.make_async_copy(refs[i], refs[count + i], sem.at[i]) for i in range(count)
    ]
    for copy in copies:
        copy.start()
    for copy in copies:
        copy.wait()


def mix_kernel(
    blocks, experts, slots, order_ref, gain_ref, fgain_ref, meta_ref, factor_ref, gate_ref,
    y_ref, cm_ref, res_ref, state_ref, *refs,
):
    count = len(blocks)
    w_refs, (mixed_ref, x_ref, send_ref) = refs[:-13], refs[-13:-10]
    wbuf, acc, vbuf, mbuf, xbuf, sbuf, sem_w, sem_m, sem_x, sem_s = refs[-10:]
    per = gate_ref.shape[1] // count
    odd = order_ref[count + 1]
    weights = []
    for i in range(count):
        weights.append([])
        for k, (which, row, size, side) in enumerate(blocks[i]):
            to = i * per
            if side is not None:
                to = to + (odd if side == 0 else 1 - odd) * size
                to = pl.multiple_of(to, size)
            copy = pltpu.make_async_copy(
                w_refs[which].at[pl.ds(row, size), :], wbuf.at[pl.ds(to, size), :], sem_w.at[i, k]
            )
            copy.start()
            weights[-1].append(copy)
    vbuf[...] = spread(factor_ref[...], gate_ref.shape[1])
    normed = []
    for i in range(count):
        wide = pl.ds(pl.multiple_of(order_ref[i] * per, per), per)
        col = pl.ds(pl.multiple_of(order_ref[i] * STATE, STATE), STATE)
        v = y_ref[:, wide] + vbuf[:, wide] * dot(cm_ref[:, col], state_ref[wide, :], 1, 1)
        v = v.astype(BF16).astype(F32)
        v = v * silu(gate_ref[:, wide].astype(F32))
        v = v * lax.rsqrt(jnp.mean(v * v, axis=1, keepdims=True) + EPS)
        normed.append((v * gain_ref[:, wide]).astype(BF16))
    features = mbuf.shape[1]
    step = features // 4
    squares = 0.0
    for i in range(0, count, 2):
        for copy in weights[i] + weights[i + 1]:
            copy.wait()
        v = jnp.concatenate(normed[i : i + 2], axis=1)
        for n in range(0, features, step):
            at = slice(n, n + step)
            out = res_ref[:, at].astype(F32) if i == 0 else acc[:, at]
            out = out + dot(v, wbuf[i * per : (i + 2) * per, at], 1, 0)
            if i < count - 2:
                acc[:, at] = out
                continue
            out = out.astype(BF16)
            mbuf[:, at] = out
            m = out.astype(F32)
            squares = squares + jnp.sum(m * m, axis=1, keepdims=True)
    out_mixed = pltpu.make_async_copy(mbuf, mixed_ref, sem_m)
    out_mixed.start()
    scale = lax.rsqrt(squares / features + EPS)
    x = (mbuf[...].astype(F32) * scale * fgain_ref[...]).astype(BF16)
    xbuf[...] = x
    out_x = pltpu.make_async_copy(xbuf, x_ref, sem_x)
    out_x.start()
    place_rows(
        hits(meta_ref[...], experts, slots, order_ref[count], send_ref.shape[0]),
        x, sbuf, send_ref, sem_s,
    )
    out_x.wait()
    out_mixed.wait()


def place_rows(hit, x, sbuf, send_ref, sem):
    pieces = sem.shape[0]
    rows = send_ref.shape[0] // pieces
    copies = []
    for i in range(pieces):
        part = slice(i * rows, (i + 1) * rows)
        sbuf[part] = dot(hit[:, part], x, 0, 0).astype(BF16)
        copies.append(
            pltpu.make_async_copy(
                sbuf.at[pl.ds(i * rows, rows)], send_ref.at[pl.ds(i * rows, rows)], sem.at[i]
            )
        )
        copies[-1].start()
    for copy in copies:
        copy.wait()


def relay_kernel(hit_ref, x_in, send_ref, x_ref, sbuf, sem_x, sem):
    pieces = sem.shape[0]
    step = x_ref.shape[1] // pieces
    wide = [pl.ds(i * step, step) for i in range(pieces)]
    gets = [pltpu.make_async_copy(x_in.at[:, w], x_ref.at[:, w], sem_x.at[i]) for i, w in enumerate(wide)]
    puts = [pltpu.make_async_copy(sbuf.at[:, w], send_ref.at[:, w], sem.at[i]) for i, w in enumerate(wide)]
    for get in gets:
        get.start()
    hit = hit_ref[...]
    for i in range(pieces):
        gets[i].wait()
        at = slice(i * step, (i + 1) * step)
        sbuf[:, at] = dot(hit, x_ref[:, at], 0, 0).astype(BF16)
        puts[i].start()
    for put in puts:
        put.wait()


def shared_kernel(x_in, mixed_in, wg_in, wu_in, wd_in, out_ref, x_ref, m_ref, wg, wu, wd, sem):
    copies = [
        pltpu.make_async_copy(src, dst, sem.at[i])
        for i, (src, dst) in enumerate(
            ((x_in, x_ref), (wg_in, wg), (wu_in, wu), (wd_in, wd), (mixed_in, m_ref))
        )
    ]
    for copy in copies:
        copy.start()
    for copy in copies[:3]:
        copy.wait()
    x = x_ref[...]
    h = (silu(dot(x, wg[...], 1, 0)) * dot(x, wu[...], 1, 0)).astype(BF16)
    for copy in copies[3:]:
        copy.wait()
    out_ref[...] = m_ref[...].astype(F32) + dot(h, wd[...], 1, 0)


def expert_kernel(x_ref, wg_ref, wu_ref, wd_ref, out_ref, hbuf, dbuf, obuf, sem, sem_d):
    e = pl.program_id(0)
    j = pl.program_id(1)
    down = pltpu.make_async_copy(wd_ref.at[e], dbuf, sem_d)

    @pl.when(j == 0)
    def _():
        down.start()

    x = x_ref[...]
    h = (silu(dot(x, wg_ref[0], 1, 0)) * dot(x, wu_ref[0], 1, 0)).astype(BF16)
    hbuf[j] = h

    @pl.when(j == pl.num_programs(1) - 1)
    def _():
        down.wait()
        hidden = jnp.concatenate([hbuf[k] for k in range(hbuf.shape[0])], axis=1)
        pieces = sem.shape[0]
        step = obuf.shape[1] // pieces
        copies = []
        for i in range(pieces):
            at = slice(i * step, (i + 1) * step)
            wide = pl.ds(i * step, step)
            obuf[:, at] = dot(hidden, dbuf[:, at], 1, 0).astype(BF16)
            copies.append(
                pltpu.make_async_copy(obuf.at[:, wide], out_ref.at[e, :, wide], sem.at[i])
            )
            copies[-1].start()
        for copy in copies:
            copy.wait()


def part_kernel(shares_ref, got_ref, out_ref, obuf, sem):
    obuf[...] = weighted(shares_ref, got_ref[...]).astype(BF16)
    copy = pltpu.make_async_copy(obuf, out_ref, sem)
    copy.start()
    copy.wait()


def sum_kernel(base_ref, other_ref, out_ref):
    out_ref[...] = base_ref[...] + other_ref[...].astype(F32)


def combine_kernel(shares_ref, got_ref, base_ref, out_ref):
    out_ref[...] = (base_ref[...] + weighted(shares_ref, got_ref[...])).astype(BF16)


def gather_rows(w, ways, span):
    if ways == 4 and w.shape[0] == 2 * span and lax.axis_size("sub") % 2 == 0:
        me = lax.axis_index("dp")
        odd = lax.rem(lax.axis_index("sub"), 2).astype(jnp.int32)
        part = span // 2
        over = [(j, j ^ 2) for j in range(4)]
        core = [(j, j ^ 1) for j in range(4)]
        flip = [(j, j ^ 1) for j in range(lax.axis_size("sub"))]
        xa = lax.ppermute(lax.dynamic_slice_in_dim(w, odd * part, part, 0), "dp", over)
        low = w[span:]
        xb = lax.ppermute(low, "dp", over)
        ya = lax.ppermute(xa, "sub", flip)
        beside = lax.ppermute(w, "dp", core)
        fa = lax.ppermute(xa, "dp", core)
        fy = lax.ppermute(ya, "dp", core)
        fb = lax.ppermute(xb, "dp", core)
        arrays = [w, beside, xa, ya, xb, fa, fy, fb]
        blocks = [[(i, k * span, span, None)] for i in range(2) for k in range(2)]
        for i in (2, 5):
            blocks.append([(i, 0, part, 0), (i + 1, 0, part, 1)])
            blocks.append([(i + 2, 0, span, None)])
        order = [(me ^ i) * 2 + k for i in range(4) for k in range(2)]
        return arrays, blocks, order, odd
    whole = lax.all_gather(w, "dp", axis=0, tiled=True)
    count = whole.shape[0] // span
    blocks = [[(0, g * span, span, None)] for g in range(count)]
    return [whole], blocks, list(range(count)), jnp.int32(0)


def layer(
    residual, head_input, gate_input, b_input, c_input, step_input, conv_weight, conv_b_weight,
    conv_c_weight, step_bias, decay_log, skip, norm_gain, out_weight, ffn_gain, shared_gate,
    shared_up, shared_down, expert_gate, expert_up, expert_down, routes, route_weights,
):
    _, tokens, inner = head_input.shape
    features = residual.shape[2]
    heads = step_input.shape[2]
    groups = b_input.shape[2] // STATE
    top = routes.shape[2]
    ways = lax.axis_size(SP)
    ways_dp = lax.axis_size("dp")
    experts = ways * ways_dp * expert_gate.shape[0]
    slots = 2 * tokens * top // experts
    local = heads // ways
    width = local * HEAD_DIM
    span = inner // groups

    ws, blocks, order, odd = gather_rows(out_weight, ways_dp, span)
    half = lax.axis_index("half").astype(jnp.int32)
    order = jnp.stack([jnp.asarray(o, jnp.int32) for o in order + [half, odd]])
    meta = jnp.concatenate([routes[0].T.astype(F32), route_weights[0].T], axis=0)
    meta = jnp.concatenate([meta, jnp.zeros((8 - 2 * top, tokens), F32)], axis=0)
    mirror = [(0, 1), (1, 0)]
    meta_far = lax.ppermute(meta, "half", mirror)
    rows = experts * slots // 2
    pieces = 4

    hbm = pl.BlockSpec(memory_space=pltpu.HBM)
    vm = pl.BlockSpec(memory_space=pltpu.VMEM)
    x_in, b_in, c_in = head_input[0], b_input[0], c_input[0]
    turned = (step_input[0].T, step_bias[None], decay_log[None])
    tail = pl.pallas_call(
        tail_kernel,
        out_shape=jax.ShapeDtypeStruct((8, inner + 2 * b_in.shape[1]), BF16),
        in_specs=[hbm] * 3,
        out_specs=vm,
        scratch_shapes=[pltpu.SemaphoreType.DMA((3,))],
        compiler_params=vmem(60),
        cost_estimate=cost(1 << 10, 1 << 17),
        name="tails",
    )(x_in, b_in, c_in)
    tail = lax.ppermute(tail, SP, [(i, i + 1) for i in range(ways - 1)])
    fresh = pl.pallas_call(
        state_kernel,
        out_shape=pltpu.HBM((ways, width + EXTRA, STATE), BF16),
        in_specs=[vm] * 8,
        out_specs=vm,
        scratch_shapes=[
            pltpu.VMEM((8 + tokens, inner), F32),
            pltpu.VMEM((8 + tokens, b_in.shape[1]), F32),
        ],
        compiler_params=vmem(24),
        cost_estimate=cost(1 << 30, 4 * MIB),
        name="states",
    )(*turned, tail, conv_weight, conv_b_weight, x_in, b_in)
    fresh = lax.all_to_all(fresh, SP, split_axis=0, concat_axis=0, tiled=True)
    y, grow, cm = pl.pallas_call(
        inner_kernel,
        out_shape=(
            pltpu.HBM((tokens, inner), F32),
            pltpu.HBM((heads, tokens), F32),
            pltpu.HBM((tokens, b_in.shape[1]), BF16),
        ),
        in_specs=[vm] * 11,
        out_specs=(vm,) * 3,
        scratch_shapes=[
            pltpu.VMEM((8 + tokens, inner), F32),
            pltpu.VMEM((8 + tokens, b_in.shape[1]), F32),
        ],
        compiler_params=vmem(24),
        cost_estimate=cost(2 << 30, 8 * MIB),
        name="within",
    )(
        *turned, skip[None], tail, conv_weight, conv_b_weight, conv_c_weight, x_in, b_in, c_in
    )
    entering = pl.pallas_call(
        prefix_kernel,
        out_shape=jax.ShapeDtypeStruct((ways, width, STATE), BF16),
        in_specs=[vm],
        out_specs=hbm,
        scratch_shapes=[pltpu.VMEM((ways, width, STATE), BF16), pltpu.SemaphoreType.DMA((ways,))],
        compiler_params=vmem(24),
        cost_estimate=cost(1 << 26, 2 * MIB),
        name="prefix",
    )(inside(fresh))
    entering = lax.all_to_all(entering, SP, split_axis=0, concat_axis=0, tiled=True)
    entering = entering.reshape(inner, STATE)

    sm = pl.BlockSpec(memory_space=pltpu.SMEM)
    warm = [gate_input[0], y, cm, residual[0]]
    warm = pl.pallas_call(
        warm_kernel,
        out_shape=tuple(pltpu.VMEM(v.shape, v.dtype) for v in warm),
        in_specs=[hbm] * len(warm),
        out_specs=(vm,) * len(warm),
        scratch_shapes=[pltpu.SemaphoreType.DMA((len(warm),))],
        compiler_params=vmem(24),
        cost_estimate=cost(1 << 28, 8 * MIB),
        name="warm",
    )(*[outside(v) for v in warm])
    warm = [inside(v) for v in warm]
    mixed, x, send = pl.pallas_call(
        functools.partial(mix_kernel, blocks, experts, slots),
        out_shape=(
            pltpu.HBM((tokens, features), BF16),
            pltpu.HBM((tokens, features), BF16),
            pltpu.HBM((rows, features), BF16),
        ),
        in_specs=[sm] + [vm] * 9 + [hbm] * len(ws),
        out_specs=(hbm, hbm, hbm),
        scratch_shapes=[
            pltpu.VMEM((groups * span, features), BF16),
            pltpu.VMEM((tokens, features), F32),
            pltpu.VMEM((tokens, inner), F32),
            pltpu.VMEM((tokens, features), BF16),
            pltpu.VMEM((tokens, features), BF16),
            pltpu.VMEM((rows, features), BF16),
            pltpu.SemaphoreType.DMA((groups, 2)),
            pltpu.SemaphoreType.DMA,
            pltpu.SemaphoreType.DMA,
            pltpu.SemaphoreType.DMA((pieces,)),
        ],
        compiler_params=vmem(36),
        cost_estimate=cost(3 << 30, 16 * MIB),
        name="mix",
    )(
        order, norm_gain[None], ffn_gain[None], meta, grow,
        *warm, inside(entering), *[outside(v) for v in ws],
    )

    x_far = lax.ppermute(x, "half", mirror)
    group = ("sub", "dp")

    def exchange(v):
        v = v.reshape(-1, slots, features)
        return lax.all_to_all(v, group, split_axis=0, concat_axis=0, tiled=True)

    own = expert_gate.shape[0]
    ff = expert_gate.shape[2]
    bn = ff // 2

    def serve(arrived):
        if own > 1:
            arrived = arrived.reshape(-1, own, slots, features).swapaxes(0, 1)
        arrived = arrived.reshape(own, -1, features)
        m = arrived.shape[1]
        done = pl.pallas_call(
            expert_kernel,
            out_shape=jax.ShapeDtypeStruct((own, m, features), BF16),
            grid=(own, ff // bn),
            in_specs=[
                pl.BlockSpec((None, m, features), lambda e, j: (e, 0, 0)),
                pl.BlockSpec((1, features, bn), lambda e, j: (e, 0, j)),
                pl.BlockSpec((1, features, bn), lambda e, j: (e, 0, j)),
                hbm,
            ],
            out_specs=hbm,
            scratch_shapes=[
                pltpu.VMEM((ff // bn, m, bn), BF16),
                pltpu.VMEM((ff, features), BF16),
                pltpu.VMEM((m, features), BF16),
                pltpu.SemaphoreType.DMA((pieces,)),
                pltpu.SemaphoreType.DMA,
            ],
            compiler_params=vmem(48),
            cost_estimate=cost(2 << 30, 8 * MIB),
            name="experts",
        )(arrived, expert_gate, expert_up, expert_down)
        if own > 1:
            done = done.reshape(own, -1, slots, features).swapaxes(0, 1)
        return done

    near = exchange(send)
    base = pl.pallas_call(
        shared_kernel,
        out_shape=jax.ShapeDtypeStruct((tokens, features), F32),
        in_specs=[hbm] * 5,
        out_specs=vm,
        scratch_shapes=[
            pltpu.VMEM(v.shape, BF16) for v in (x, mixed, shared_gate, shared_up, shared_down)
        ]
        + [pltpu.SemaphoreType.DMA((5,))],
        compiler_params=vmem(62),
        cost_estimate=cost(1 << 30, 8 * MIB),
        name="shared",
    )(x, mixed, shared_gate, shared_up, shared_down)
    near = serve(near)
    hit_far, near_shares, far_shares = pl.pallas_call(
        functools.partial(plan_kernel, experts, slots),
        out_shape=(
            jax.ShapeDtypeStruct((tokens, rows), BF16),
            jax.ShapeDtypeStruct((2, tokens, rows), BF16),
            jax.ShapeDtypeStruct((2, tokens, rows), BF16),
        ),
        in_specs=[sm, vm, vm],
        out_specs=(vm,) * 3,
        compiler_params=vmem(24),
        cost_estimate=cost(1 << 27, 1 << 19),
        name="plan",
    )(half[None], meta, meta_far)
    relay = pl.pallas_call(
        relay_kernel,
        out_shape=pltpu.HBM((rows, features), BF16),
        in_specs=[vm, hbm],
        out_specs=hbm,
        scratch_shapes=[
            pltpu.VMEM((tokens, features), BF16),
            pltpu.VMEM((rows, features), BF16),
            pltpu.SemaphoreType.DMA((pieces,)),
            pltpu.SemaphoreType.DMA((pieces,)),
        ],
        compiler_params=vmem(32),
        cost_estimate=cost(1 << 28, 3 * MIB),
        name="relay",
    )(hit_far, x_far)
    far = exchange(relay)
    far = serve(far)
    far = exchange(far)
    part = pl.pallas_call(
        part_kernel,
        out_shape=pltpu.HBM((tokens, features), BF16),
        in_specs=[vm, vm],
        out_specs=hbm,
        scratch_shapes=[pltpu.VMEM((tokens, features), BF16), pltpu.SemaphoreType.DMA],
        compiler_params=vmem(32),
        cost_estimate=cost(1 << 29, 3 * MIB),
        name="part",
    )(far_shares, far.reshape(rows, features))
    other = lax.ppermute(part, "half", mirror)
    near = exchange(near)
    base = pl.pallas_call(
        sum_kernel,
        out_shape=jax.ShapeDtypeStruct((tokens, features), F32),
        in_specs=[vm, vm],
        out_specs=vm,
        compiler_params=vmem(32),
        cost_estimate=cost(1 << 20, 3 * MIB),
        name="sum",
    )(base, other)
    out = pl.pallas_call(
        combine_kernel,
        out_shape=jax.ShapeDtypeStruct((tokens, features), BF16),
        in_specs=[vm] * 3,
        out_specs=vm,
        compiler_params=vmem(32),
        cost_estimate=cost(1 << 29, 4 * MIB),
        name="combine",
    )(near_shares, near.reshape(rows, features), base)
    return out[None]


def solution(mesh):
    ways, ways_dp = mesh.devices.shape
    mesh = jax.sharding.Mesh(mesh.devices.reshape(2, ways // 2, ways_dp), SP + ("dp",))
    tok = P("dp", SP, None)
    exp = P(SP + ("dp",), None, None)
    return jax.shard_map(
        layer,
        mesh=mesh,
        in_specs=(tok,) * 6
        + (P(),) * 7
        + (P("dp", None),)
        + (P(),) * 4
        + (exp,) * 3
        + (tok, tok),
        out_specs=tok,
        check_vma=False,
    )
```
